128 devices in a mesh: rep: 2 (over z_hi), fs: 32 (over z_lo, y, x), tp: 2 (over core).
Axes of the slice: x: 4, y: 4, z: 4 (z_hi: 2, z_lo: 2; z = z_hi * 2 + z_lo), core: 2. Of those that a mesh axis runs over, the one named last changes fastest.
Arguments:
- stream_in: bfloat16 [64, 1024, 2048], P(('rep', 'fs'), None, 'tp'), may hold values from -48 to 48
- decay_shift: float32 [64, 1024], P(('rep', 'fs')), may hold values from -1.5 to 0, as said below
- mixer_gain: float32 [2048], replicated, may hold values from 0.1 to 1.9
- gate_weight: bfloat16 [2048, 1024], P('fs', 'tp'), may hold values from -0.125 to 0.125
- input_weight: bfloat16 [2048, 1024], P('fs', 'tp'), may hold values from -0.125 to 0.125
- filter_taps: float32 [4, 1024], P(None, 'tp'), may hold values from -3 to 3
- recur_gate: bfloat16 [4, 256, 256], P('tp'), may hold values from -0.375 to 0.375
- inlet_gate: bfloat16 [4, 256, 256], P('tp'), may hold values from -0.375 to 0.375
- decay_param: float32 [1024], P('tp'), may hold values from 1.5 to 12
- mixer_out: bfloat16 [1024, 2048], P('tp', 'fs'), may hold values from -0.1875 to 0.1875
- feedforward_gain: float32 [2048], replicated, may hold values from 0.1 to 1.9
- up_weight: bfloat16 [2048, 4096], P('fs', 'tp'), may hold values from -0.125 to 0.125
- down_weight: bfloat16 [4096, 2048], P('tp', 'fs'), may hold values from -0.09375 to 0.09375
- final_gain: float32 [2048], P('tp'), may hold values from 0.1 to 1.9
Outputs:
- layer_out: bfloat16 [64, 1024, 2048], P(('rep', 'fs'), None, 'tp')
The draws below stay inside these ranges and needn't reach their ends.
Inputs may be any that keep to these rules, and one draw needn't show every extreme that they name: `decay_shift`: every entry is negative.
All inputs are finite; a program needn't handle non-finite values.
Results may differ from the reference program's by a relative error of at most 0.015.
Values may be sent and summed in bfloat16 or wider, within the bound.
No kernel may reach another device: no remote copies, remote signals or barrier semaphores. Data moves between devices by JAX's collectives and lax.ppermute only.
A program may use at most 128 MiB of HBM per device.

```python
import math
import jax
import jax.numpy as jnp
from jax import lax

D = 2048
NB = 4
BLOCK = 256
DR = 1024
FF = 4096
TAPS = 4
LENGTH = 1024
SEQS = 64
N_TP = 2


def draw_stream_in(key, part):
    starting_level = jax.random.normal(jax.random.fold_in(key, 1), (SEQS, LENGTH, D), jnp.float32)
    ramp = jnp.exp(jnp.linspace(math.log(0.5), math.log(2.0), D)).astype(jnp.float32)
    lower, upper = (math.log(0.5), math.log(2.0))
    row_scale = jnp.exp(jax.random.uniform(jax.random.fold_in(key, 2), (SEQS, LENGTH, 1), jnp.float32, lower, upper))
    return (jnp.clip(starting_level, -6.0, 6.0) * ramp[None, None, :] * row_scale).astype(jnp.bfloat16)


def draw_decay_param(key, part):
    fast_cut = 5
    fast = jax.random.randint(jax.random.fold_in(key, 11), (DR,), 0, 10) < fast_cut
    keep = jnp.exp(jax.random.uniform(jax.random.fold_in(key, 12), (DR,), jnp.float32, math.log(0.4), math.log(0.9)))
    slow_rate = -jnp.log(keep) / LENGTH
    short_span = float(min(30, LENGTH // 4))
    long_span = float(min(100, LENGTH // 2))
    fast_rate = 2.3 / jax.random.uniform(jax.random.fold_in(key, 13), (DR,), jnp.float32, short_span, long_span)
    rate = jnp.where(fast, fast_rate, slow_rate) / (8.0 * 0.5)
    return (-jnp.log(jnp.expm1(rate))).astype(jnp.float32)


def draw_decay_shift(key, part):
    starting_level = -jnp.exp(jax.random.uniform(jax.random.fold_in(key, 21), (SEQS, 1), jnp.float32, math.log(0.105), math.log(0.69))) / LENGTH
    spots = jax.random.randint(jax.random.fold_in(key, 22), (SEQS, 2), 0, LENGTH)
    number_of_tiers = jnp.log(jax.random.uniform(jax.random.fold_in(key, 23), (SEQS, 2), jnp.float32, 0.5, 0.8))
    places = jnp.arange(LENGTH, dtype=jnp.int32)
    agreement_tally = (places[None, None, :] == spots[:, :, None]).astype(jnp.float32)
    spike_source = jnp.sum(agreement_tally * number_of_tiers[:, :, None], axis=1)
    return (starting_level + spike_source).astype(jnp.float32)


def block_scale(own_key, dims, split, smallest, high):
    gain, own = 1.0, jax.random.fold_in(own_key, 6)
    for axis_at, shards_of in split:
        steps = jnp.exp(jax.random.uniform(jax.random.fold_in(own, axis_at), (shards_of,), jnp.float32, smallest / len(split), high / len(split)))
        gain = gain * jnp.repeat(steps, dims[axis_at] // shards_of).reshape([-1 if axis == axis_at else 1 for axis in range(len(dims))])
    return gain


def normal_values(own_key, shape, width, bound, split=(), kind=jnp.bfloat16):
    entries = width * jax.random.normal(own_key, shape, jnp.float32)
    if split:
        entries = entries * block_scale(own_key, shape, split, -0.22, 0.18)
    return jnp.clip(entries, -bound, bound).astype(kind)


def setup_inputs(seed: int = 0) -> dict:
    key_of = jax.random.split(jax.random.key(seed), 15)
    return {
        "stream_in": draw_stream_in(jax.random.fold_in(key_of[14], 71), 0),
        "decay_shift": draw_decay_shift(jax.random.fold_in(key_of[14], 71), 0),
        "mixer_gain": jnp.clip(1.0 + 0.18 * jax.random.normal(key_of[2], (D,), jnp.float32), 0.1, 1.9),
        "gate_weight": normal_values(key_of[3], (D, DR), D ** -0.5, 0.125, ((0, 32), (1, 2))),
        "input_weight": normal_values(key_of[4], (D, DR), D ** -0.5, 0.125, ((0, 32), (1, 2))),
        "filter_taps": normal_values(key_of[5], (TAPS, DR), 0.5, 3.0, ((1, 2),), jnp.float32),
        "recur_gate": normal_values(key_of[6], (NB, BLOCK, BLOCK), BLOCK ** -0.5, 0.375, ((0, 2),)),
        "inlet_gate": normal_values(key_of[7], (NB, BLOCK, BLOCK), BLOCK ** -0.5, 0.375, ((0, 2),)),
        "decay_param": draw_decay_param(jax.random.fold_in(key_of[14], 71), 0),
        "mixer_out": normal_values(key_of[9], (DR, D), DR ** -0.5, 0.1875, ((0, 2), (1, 32))),
        "feedforward_gain": jnp.clip(1.0 + 0.18 * jax.random.normal(key_of[10], (D,), jnp.float32), 0.1, 1.9),
        "up_weight": normal_values(key_of[11], (D, FF), D ** -0.5, 0.125, ((0, 32), (1, 2))),
        "down_weight": normal_values(key_of[12], (FF, D), FF ** -0.5, 0.09375, ((0, 2), (1, 32))),
        "final_gain": jnp.clip(1.0 + 0.18 * jax.random.normal(key_of[13], (D,), jnp.float32), 0.1, 1.9),
    }


epsilon = 1e-06
rate_scale = 8.0

def norm_rows(values, row_gain):
    mean_sq = lax.optimization_barrier(jnp.mean(values * values, axis=-1, keepdims=True))
    return values * lax.rsqrt(mean_sq + epsilon) * row_gain

def split_sum(left, right):
    share = right.shape[0] // N_TP
    total = jnp.zeros((left.shape[0], right.shape[1]), jnp.float32)
    for index in range(N_TP):
        partial_prod = jnp.dot(left[:, index * share:(index + 1) * share], right[index * share:(index + 1) * share], preferred_element_type=jnp.float32)
        rounded = lax.optimization_barrier(partial_prod.astype(jnp.bfloat16))
        total = total + rounded.astype(jnp.float32)
    return total

def combine(earlier, later):
    return (earlier[0] * later[0], later[0] * earlier[1] + later[1])

def reference(stream_in, decay_shift, mixer_gain, gate_weight, input_weight, filter_taps, recur_gate, inlet_gate, decay_param, mixer_out, feedforward_gain, up_weight, down_weight, final_gain):

    def one_sequence(inputs):
        seq_in, shift_row = inputs
        length = seq_in.shape[0]
        stream_f = seq_in.astype(jnp.float32)
        normed = norm_rows(stream_f, mixer_gain).astype(jnp.bfloat16)
        gate_logits = jnp.dot(normed, gate_weight, preferred_element_type=jnp.float32).astype(jnp.bfloat16)
        input_pre = jnp.dot(normed, input_weight, preferred_element_type=jnp.float32).astype(jnp.bfloat16)
        branch = jax.nn.gelu(gate_logits.astype(jnp.float32), approximate=True)
        extended_front = jnp.pad(input_pre.astype(jnp.float32), ((TAPS - 1, 0), (0, 0)))
        filtered = jnp.zeros(input_pre.shape, jnp.float32)
        for offset in range(TAPS):
            filtered = filtered + extended_front[offset:offset + length] * filter_taps[offset][None, :]
        filtered = filtered.astype(jnp.bfloat16)
        grouped = filtered.astype(jnp.float32).reshape(length, NB, BLOCK)
        recur = jax.nn.sigmoid(jnp.einsum('lni,nij->lnj', grouped, recur_gate.astype(jnp.float32)).reshape(length, DR))
        inlet = jax.nn.sigmoid(jnp.einsum('lni,nij->lnj', grouped, inlet_gate.astype(jnp.float32)).reshape(length, DR))
        logarithm_decay = -rate_scale * recur * jax.nn.softplus(-decay_param)[None, :] + shift_row[:, None]
        decay = jnp.exp(logarithm_decay)
        drive = jnp.sqrt(-jnp.expm1(2.0 * logarithm_decay)) * inlet * filtered.astype(jnp.float32)
        states = lax.associative_scan(combine, (decay, drive), axis=0)[1]
        mixed = (states * branch).astype(jnp.bfloat16)
        mixer_sum = split_sum(mixed, mixer_out)
        stream_mid = (stream_f + mixer_sum).astype(jnp.bfloat16)
        normed_mid = norm_rows(stream_mid.astype(jnp.float32), feedforward_gain).astype(jnp.bfloat16)
        up_proj = jnp.dot(normed_mid, up_weight, preferred_element_type=jnp.float32)
        activated = jnp.square(jax.nn.relu(up_proj)).astype(jnp.bfloat16)
        ffn_sum = split_sum(activated, down_weight)
        total = stream_mid.astype(jnp.float32) + ffn_sum
        return norm_rows(total, final_gain).astype(jnp.bfloat16)
    return lax.map(one_sequence, (stream_in, decay_shift))
```

```python
import functools

import jax
import jax.numpy as jnp
from jax import lax
from jax.experimental import pallas as pl
from jax.experimental.pallas import tpu as pltpu
from jax.sharding import Mesh, PartitionSpec as P

D = 2048
HALF = 1024
ROWS = 64
TILE = 256
SEGS = 8

epsilon = 1e-06
rate_scale = 8.0


f32, bf16 = jnp.float32, jnp.bfloat16
VMEM = pl.BlockSpec(memory_space=pltpu.VMEM)
HBM = pl.BlockSpec(memory_space=pltpu.HBM)
SMEM = pl.BlockSpec(memory_space=pltpu.SMEM)


def step(v, axis, shift):
    size = 2 if axis == "tp" else 4
    name = ("rep", "z") if axis == "z" else axis
    return lax.ppermute(v, name, [(i, (i + shift) % size) for i in range(size)])


def moved(places, axis, by):
    at = "xyz".index(axis)
    return [p[:at] + (p[at] + by,) + p[at + 1 :] for p in places]


def both_planes(shard):
    half = shard.shape[0] // 2
    lower = step(shard[:half], "z", 1)
    upper = step(shard[half:], "z", 3)
    pair = jnp.stack([shard, jnp.concatenate([lower, upper], axis=0)])
    return pair, [(0, 0, 0, 0, 0), (0, 0, 1, 0, 0)]


def whole_ring(v, places, axis):
    parts = [v, step(v, axis, 1), step(v, axis, 3), step(v, axis, 2)]
    out = sum((moved(places, axis, by) for by in (0, -1, 1, 2)), [])
    return jnp.concatenate(parts, axis=0), out


def ring_pieces(v, places, axis):
    mid = v.shape[0] // 2
    left = step(v, axis, 1)
    right = step(v, axis, 3)
    far_low = step(left[:mid], axis, 1)
    far_high = step(right[mid:], axis, 3)
    return [
        (v, places),
        (left, moved(places, axis, -1)),
        (right, moved(places, axis, 1)),
        (far_low, moved(places, axis, 2)[:mid]),
        (far_high, moved(places, axis, 2)[mid:]),
    ]


def plane_then_other(shard, shift, first_row):
    own = lax.all_gather(shard, ("y", "x"), axis=0, tiled=False)
    other = step(own, "z", shift)
    return [
        (own, [(i % 4, i // 4, 0, 1, first_row) for i in range(16)]),
        (other, [(i % 4, i // 4, 1, 1, first_row) for i in range(16)]),
    ]


def start_weights(refs, layout, pos, target, sem):
    x, y, z, tp = pos[0], pos[1], pos[2], pos[3]
    for ref, (places, first_col, width) in zip(refs, layout):
        rows = ref.shape[1]
        for b, (px, py, pz, absolute, first_row) in enumerate(places):
            line = (py * 4 + px) if absolute else ((y + py) & 3) * 4 + ((x + px) & 3)
            at = (((z + pz) & 1) * 16 + line) * ROWS + first_row
            at = pl.multiple_of((at + tp * HALF) & (D - 1), 16)
            pltpu.make_async_copy(
                ref.at[b], target.at[pl.ds(at, rows), pl.ds(first_col, width)], sem
            ).start()


def norm_kernel(own, other, gain, normed):
    def rows(i, _):
        s = pl.ds(pl.multiple_of(i * TILE, TILE), TILE)
        a, b = own[s, :].astype(f32), other[s, :].astype(f32)
        ms = (jnp.sum(a * a, -1, keepdims=True) + jnp.sum(b * b, -1, keepdims=True)) / D
        r = lax.rsqrt(ms + epsilon)
        normed[s, :HALF] = (a * r * gain[:, :HALF]).astype(bf16)
        normed[s, HALF:] = (b * r * gain[:, HALF:]).astype(bf16)
        return 0

    lax.fori_loop(0, own.shape[0] // TILE, rows, 0)


def mixer_kernel(layout, *refs):
    n = len(layout)
    pos, normed, taps, recur_gate, inlet_gate, rate, shift = refs[:7]
    pieces, mixed = refs[7 : 7 + n], refs[7 + n]
    weights, gate, padded, decay, drive, prod, sem = refs[8 + n :]
    length, channels = mixed.shape
    start_weights(pieces, layout, pos, weights, sem)
    padded[:8, :] = jnp.zeros((8, channels), f32)
    pltpu.make_async_copy(weights, weights, sem).wait()
    blocks, block = recur_gate.shape[0], recur_gate.shape[1]
    for r in range(0, length, TILE):
        x = normed[r : r + TILE, :]
        gate[r : r + TILE, :] = jnp.dot(
            x, weights[:, :channels], preferred_element_type=f32
        ).astype(bf16)
        padded[8 + r : 8 + r + TILE, :] = (
            jnp.dot(x, weights[:, channels:], preferred_element_type=f32).astype(bf16).astype(f32)
        )
    for r in range(0, length, TILE):
        acc = padded[r + 5 : r + 5 + TILE, :] * taps[0:1, :]
        for k in range(1, 4):
            acc = acc + padded[r + 5 + k : r + 5 + k + TILE, :] * taps[k : k + 1, :]
        filt = acc.astype(bf16)
        for n_b in range(blocks):
            cols = slice(n_b * block, (n_b + 1) * block)
            fb = filt[:, cols]
            recur = jax.nn.sigmoid(jnp.dot(fb, recur_gate[n_b], preferred_element_type=f32))
            inlet = jax.nn.sigmoid(jnp.dot(fb, inlet_gate[n_b], preferred_element_type=f32))
            log_decay = shift[r : r + TILE, :] - recur * rate[:, cols]
            a = jnp.exp(log_decay)
            t = 2.0 * log_decay
            series = -t * (
                1.0
                + t
                * (
                    1.0 / 2
                    + t
                    * (1.0 / 6 + t * (1.0 / 24 + t * (1.0 / 120 + t * (1.0 / 720 + t / 5040))))
                )
            )
            gone = jnp.where(t > -0.4, series, 1.0 - a * a)
            into = jnp.sqrt(gone) * inlet * fb.astype(f32)
            for q in range(block // 128):
                at = n_b * (block // 128) + q
                decay[at, r : r + TILE, :] = a[:, q * 128 : q * 128 + 128]
                drive[at, r : r + TILE, :] = into[:, q * 128 : q * 128 + 128]
    seg = length // SEGS

    def scan(j, carry):
        h, p = carry
        s = pl.ds(j, SEGS, stride=seg)
        hs, ps = [], []
        for q in range(channels // 128):
            a = decay[q, s, :]
            hq = a * h[q] + drive[q, s, :]
            pq = a * p[q]
            drive[q, s, :] = hq
            prod[q, s, :] = pq
            hs.append(hq)
            ps.append(pq)
        return tuple(hs), tuple(ps)

    lanes = channels // 128
    zero, one = jnp.zeros((SEGS, 128), f32), jnp.ones((SEGS, 128), f32)
    lax.fori_loop(0, seg, scan, ((zero,) * lanes, (one,) * lanes), unroll=8)
    for q in range(lanes):
        carry = jnp.zeros((1, 128), f32)
        for i in range(SEGS):
            s = slice(i * seg, (i + 1) * seg)
            cols = slice(q * 128, q * 128 + 128)
            states = drive[q, s, :] + prod[q, s, :] * carry
            carry = states[seg - 1 : seg, :]
            branch = jax.nn.gelu(gate[s, cols].astype(f32), approximate=True)
            mixed[s, cols] = (states * branch).astype(bf16)


def turned_kernel(layout, *refs):
    n = len(layout)
    pos, left = refs[:2]
    pieces, out = refs[2 : 2 + n], refs[2 + n]
    weights, sem = refs[3 + n :]
    start_weights(pieces, layout, pos, weights, sem)
    pltpu.make_async_copy(weights, weights, sem).wait()
    for r in range(0, out.shape[0], TILE):
        out[r : r + TILE, :] = lax.dot_general(
            left[r : r + TILE, :],
            weights[...],
            (((1,), (1,)), ((), ())),
            preferred_element_type=f32,
        ).astype(bf16)


def middle_kernel(own, other, mine, theirs, gain, mid, normed):
    def rows(i, _):
        s = pl.ds(pl.multiple_of(i * TILE, TILE), TILE)
        a = own[s, :].astype(f32) + (
            mine[s, :HALF].astype(f32) + theirs[s, HALF:].astype(f32)
        )
        b = other[s, :].astype(f32) + (
            mine[s, HALF:].astype(f32) + theirs[s, :HALF].astype(f32)
        )
        a, b = a.astype(bf16), b.astype(bf16)
        mid[s, :HALF] = a
        mid[s, HALF:] = b
        a, b = a.astype(f32), b.astype(f32)
        ms = (jnp.sum(a * a, -1, keepdims=True) + jnp.sum(b * b, -1, keepdims=True)) / D
        r = lax.rsqrt(ms + epsilon)
        normed[s, :HALF] = (a * r * gain[:, :HALF]).astype(bf16)
        normed[s, HALF:] = (b * r * gain[:, HALF:]).astype(bf16)
        return 0

    lax.fori_loop(0, own.shape[0] // TILE, rows, 0)


def up_kernel(layout, *refs):
    n = len(layout)
    pos, left = refs[:2]
    pieces, out = refs[2 : 2 + n], refs[2 + n]
    weights, sem = refs[3 + n :]
    start_weights(pieces, layout, pos, weights, sem)
    pltpu.make_async_copy(weights, weights, sem).wait()
    for r in range(0, out.shape[0], TILE):
        prod = jnp.dot(left[r : r + TILE, :], weights[...], preferred_element_type=f32)
        out[r : r + TILE, :] = jnp.square(jnp.maximum(prod, 0.0)).astype(bf16)


def closing_kernel(mid, mine, theirs, gain, out):
    def rows(i, _):
        s = pl.ds(pl.multiple_of(i * TILE, TILE), TILE)
        a = mid[s, :HALF].astype(f32) + (
            mine[s, :HALF].astype(f32) + theirs[s, HALF:].astype(f32)
        )
        b = mid[s, HALF:].astype(f32) + (
            mine[s, HALF:].astype(f32) + theirs[s, :HALF].astype(f32)
        )
        ms = (jnp.sum(a * a, -1, keepdims=True) + jnp.sum(b * b, -1, keepdims=True)) / D
        out[s, :] = (a * lax.rsqrt(ms + epsilon) * gain[...]).astype(bf16)
        return 0

    lax.fori_loop(0, out.shape[0] // TILE, rows, 0)


def cost(flops, moved_bytes):
    return pl.CostEstimate(flops=int(flops), bytes_accessed=int(moved_bytes), transcendentals=0)


def call(kernel, out_shapes, specs, name, flops, scratch=(), outs=VMEM):
    return pl.pallas_call(
        kernel,
        out_shape=out_shapes,
        in_specs=specs,
        out_specs=jax.tree.map(lambda _: outs, out_shapes),
        scratch_shapes=list(scratch),
        cost_estimate=cost(flops, 8e6),
        name=name,
        compiler_params=pltpu.CompilerParams(vmem_limit_bytes=56 * 2**20),
    )


def flat(pieces, first_col, width):
    return [v for v, _ in pieces], [(places, first_col, width) for _, places in pieces]


def local(
    stream_in,
    decay_shift,
    mixer_gain,
    gate_weight,
    input_weight,
    filter_taps,
    recur_gate,
    inlet_gate,
    decay_param,
    mixer_out,
    feedforward_gain,
    up_weight,
    down_weight,
    final_gain,
):
    num_seq, length, half = stream_in.shape
    channels = gate_weight.shape[1]
    hidden = up_weight.shape[1]
    assert num_seq == 1 and half == HALF
    tp = lax.axis_index("tp")
    pos = jnp.stack(
        [lax.axis_index("x"), lax.axis_index("y"), lax.axis_index("z"), tp]
    ).astype(jnp.int32)

    def own_first(gain):
        halves = gain.reshape(2, HALF)
        return jnp.where(tp == 0, halves, halves[::-1]).reshape(1, D)

    own = stream_in.reshape(length, half)
    other = step(own, "tp", 1)

    pair, places = both_planes(jnp.concatenate([gate_weight, input_weight, up_weight], axis=1))
    cut = channels + channels
    mid_col = cut + hidden // 2
    by_x = whole_ring(pair[:, :, :channels], places, "y")
    by_y = whole_ring(pair[:, :, channels:cut], places, "x")
    gate_pieces = ring_pieces(*by_x, "x")
    input_pieces = ring_pieces(*by_y, "y")
    out_pieces = []
    mixer_t = mixer_out.T
    plane = lax.all_gather(mixer_t, ("y", "x"), axis=0, tiled=False)
    lower, upper = step(plane[:8], "z", 1), step(plane[8:], "z", 3)
    spots = [(i % 4, i // 4, 0, 1, 0) for i in range(16)]
    out_pieces = [
        (plane, spots),
        (lower, moved(spots[:8], "z", 1)),
        (upper, moved(spots[8:], "z", 1)),
    ]
    up_x = ring_pieces(*whole_ring(pair[:, :, cut:mid_col], places, "y"), "x")
    up_y = ring_pieces(*whole_ring(pair[:, :, mid_col:], places, "x"), "y")
    down_t = down_weight.T
    down_pieces = plane_then_other(down_t[: ROWS // 2], 1, 0) + plane_then_other(
        down_t[ROWS // 2 :], 3, ROWS // 2
    )

    shape = jax.ShapeDtypeStruct
    normed = call(norm_kernel, shape((length, D), bf16), [VMEM] * 3, "norm", 2e9)(
        own, other, own_first(mixer_gain)
    )

    a, la = flat(gate_pieces, 0, channels)
    b, lb = flat(input_pieces, channels, channels)
    mixed = call(
        functools.partial(mixer_kernel, la + lb),
        shape((length, channels), bf16),
        [SMEM] + [VMEM] * 6 + [HBM] * len(la + lb),
        "mixer",
        1e10,
        [
            pltpu.VMEM((D, 2 * channels), bf16),
            pltpu.VMEM((length, channels), bf16),
            pltpu.VMEM((length + 8, channels), f32),
            pltpu.VMEM((channels // 128, length, 128), f32),
            pltpu.VMEM((channels // 128, length, 128), f32),
            pltpu.VMEM((channels // 128, length, 128), f32),
            pltpu.SemaphoreType.DMA,
        ],
    )(
        pos,
        normed,
        filter_taps,
        recur_gate,
        inlet_gate,
        (rate_scale * jax.nn.softplus(-decay_param)).reshape(1, channels),
        decay_shift.reshape(length, 1),
        *a,
        *b,
    )

    def turned(left, pieces, name):
        arrays, layout = flat(pieces, 0, left.shape[1])
        return call(
            functools.partial(turned_kernel, layout),
            shape((length, D), bf16),
            [SMEM, VMEM] + [HBM] * len(layout),
            name,
            2 * length * left.shape[1] * D,
            [pltpu.VMEM((D, left.shape[1]), bf16), pltpu.SemaphoreType.DMA],
        )(pos, left, *arrays)

    mine = turned(mixed, out_pieces, "mixer_out")
    theirs = step(mine, "tp", 1)
    mid, normed_mid = call(
        middle_kernel,
        (shape((length, D), bf16), shape((length, D), bf16)),
        [VMEM] * 5,
        "middle",
        2e9,
    )(own, other, mine, theirs, own_first(feedforward_gain))
    a, la = flat(up_x, 0, hidden // 2)
    b, lb = flat(up_y, hidden // 2, hidden // 2)
    activated = call(
        functools.partial(up_kernel, la + lb),
        shape((length, hidden), bf16),
        [SMEM, VMEM] + [HBM] * len(la + lb),
        "up",
        2 * length * hidden * D,
        [pltpu.VMEM((D, hidden), bf16), pltpu.SemaphoreType.DMA],
    )(pos, normed_mid, *a, *b)
    mine = turned(activated, down_pieces, "down")
    theirs = step(mine, "tp", 1)
    out = call(closing_kernel, shape((length, HALF), bf16), [VMEM] * 4, "closing", 2e9)(
        mid, mine, theirs, final_gain.reshape(1, HALF)
    )
    return out.reshape(num_seq, length, half)


def solution(mesh):
    grid = Mesh(mesh.devices.reshape(2, 2, 4, 4, 2), ("rep", "z", "y", "x", "tp"))
    fs = ("z", "y", "x")
    seqs = ("rep",) + fs
    return jax.shard_map(
        local,
        mesh=grid,
        in_specs=(
            P(seqs, None, "tp"),
            P(seqs, None),
            P(),
            P(fs, "tp"),
            P(fs, "tp"),
            P(None, "tp"),
            P("tp", None, None),
            P("tp", None, None),
            P("tp"),
            P("tp", fs),
            P(),
            P(fs, "tp"),
            P("tp", fs),
            P("tp"),
        ),
        out_specs=P(seqs, None, "tp"),
        check_vma=False,
    )
```

```python
import functools

import jax
import jax.numpy as jnp
from jax import lax
from jax.experimental import pallas as pl
from jax.experimental.pallas import tpu as pltpu
from jax.sharding import Mesh, PartitionSpec as P

D = 2048
HALF = 1024
ROWS = 64
TILE = 256
SEGS = 8

epsilon = 1e-06
rate_scale = 8.0


f32, bf16 = jnp.float32, jnp.bfloat16
VMEM = pl.BlockSpec(memory_space=pltpu.VMEM)
HBM = pl.BlockSpec(memory_space=pltpu.HBM)
SMEM = pl.BlockSpec(memory_space=pltpu.SMEM)


def step(v, axis, shift):
    size = 2 if axis == "tp" else 4
    over = ("rep", "z") if axis == "z" else axis
    return lax.ppermute(v, over, [(i, (i + shift) % size) for i in range(size)])


def moved(places, axis, by):
    at = "xyz".index(axis)
    return [p[:at] + (p[at] + by,) + p[at + 1 :] for p in places]


def both_planes(shard):
    half = shard.shape[0] // 2
    lower = step(shard[:half], "z", 1)
    upper = step(shard[half:], "z", 3)
    pair = jnp.stack([shard, jnp.concatenate([lower, upper], axis=0)])
    return pair, [(0, 0, 0, 0, 0), (0, 0, 1, 0, 0)]


def ring_pieces(v, places, axis):
    far = step(v, axis, 2)
    left = step(v, axis, 1)
    right = step(v, axis, 3)
    return [
        (v, places),
        (left, moved(places, axis, -1)),
        (right, moved(places, axis, 1)),
        (far, moved(places, axis, 2)),
    ]


def whole_ring(v, places, axis):
    pieces = ring_pieces(v, places, axis)
    return jnp.concatenate([p for p, _ in pieces], axis=0), sum((q for _, q in pieces), [])


def plane_pieces(own, first, width):
    half = own.shape[0] // 2
    places = [(i % 4, i // 4, 0, 1, 0) for i in range(2 * half)]
    lower = step(own[:half, :, first : first + width], "z", 1)
    upper = step(own[half:, :, first : first + width], "z", 3)
    far = moved(places, "z", 1)
    return [(own, places, first), (lower, far[:half]), (upper, far[half:])]


def start_weights(refs, layout, pos, target, sem, plane=None):
    x, y, z, tp = pos[0], pos[1], pos[2], pos[3]
    for ref, (places, first_col, width, source_col) in zip(refs, layout):
        cols, source = pl.ds(first_col, width), pl.ds(source_col, width)
        for b, (px, py, pz, absolute, first_row) in enumerate(places):
            line = (py * 4 + px) if absolute else ((y + py) & 3) * 4 + ((x + px) & 3)
            at = line * ROWS + first_row
            if plane is None:
                at = ((z + pz + tp) & 1) * HALF + at
            elif pz != plane:
                continue
            at = at if isinstance(at, int) else pl.multiple_of(at, 16)
            pltpu.make_async_copy(
                ref.at[b, :, source], target.at[pl.ds(at, ref.shape[1]), cols], sem
            ).start()


def norm_kernel(own, other, gain, normed):
    def rows(i, _):
        s = pl.ds(pl.multiple_of(i * TILE, TILE), TILE)
        a, b = own[s, :].astype(f32), other[s, :].astype(f32)
        ms = (jnp.sum(a * a, -1, keepdims=True) + jnp.sum(b * b, -1, keepdims=True)) / D
        r = lax.rsqrt(ms + epsilon)
        normed[s, :HALF] = (a * r * gain[:, :HALF]).astype(bf16)
        normed[s, HALF:] = (b * r * gain[:, HALF:]).astype(bf16)
        return 0

    lax.fori_loop(0, own.shape[0] // TILE, rows, 0)


def project_kernel(layout, *refs):
    n = len(layout)
    pos, normed = refs[:2]
    pieces, (gate, inner) = refs[2 : 2 + n], refs[2 + n : 4 + n]
    weights, sem = refs[4 + n :]
    length, channels = gate.shape
    start_weights(pieces, layout, pos, weights, sem)
    pltpu.make_async_copy(weights, weights, sem).wait()
    for r in range(0, length, TILE):
        x = normed[r : r + TILE, :]
        both = jnp.dot(x, weights[...], preferred_element_type=f32).astype(bf16)
        gate[r : r + TILE, :] = both[:, :channels]
        inner[r : r + TILE, :] = both[:, channels:]


def mixer_kernel(layout, *refs):
    n = len(layout)
    pos, gate, inner, taps, recur_gate, inlet_gate, rate, shift = refs[:8]
    pieces, part_out = refs[8 : 8 + n], refs[8 + n]
    padded, decay, drive, prod, weights, part, weight_sem, out_sem = refs[9 + n :]
    length, channels = gate.shape
    start_weights(pieces, layout, pos, weights, weight_sem)
    padded[:8, :] = jnp.zeros((8, channels), f32)
    blocks, block = recur_gate.shape[0], recur_gate.shape[1]
    for r in range(0, length, TILE):
        padded[8 + r : 8 + r + TILE, :] = inner[r : r + TILE, :].astype(f32)
        acc = padded[r + 5 : r + 5 + TILE, :] * taps[0:1, :]
        for k in range(1, 4):
            acc = acc + padded[r + 5 + k : r + 5 + k + TILE, :] * taps[k : k + 1, :]
        filt = acc.astype(bf16)
        for n_b in range(blocks):
            cols = slice(n_b * block, (n_b + 1) * block)
            fb = filt[:, cols]
            recur = jax.nn.sigmoid(jnp.dot(fb, recur_gate[n_b], preferred_element_type=f32))
            inlet = jax.nn.sigmoid(jnp.dot(fb, inlet_gate[n_b], preferred_element_type=f32))
            log_decay = shift[r : r + TILE, :] - recur * rate[:, cols]
            a = jnp.exp(log_decay)
            t = 2.0 * log_decay
            series = -t * (
                1.0
                + t
                * (
                    1.0 / 2
                    + t
                    * (1.0 / 6 + t * (1.0 / 24 + t * (1.0 / 120 + t * (1.0 / 720 + t / 5040))))
                )
            )
            gone = jnp.where(t > -0.4, series, 1.0 - a * a)
            into = jnp.sqrt(gone) * inlet * fb.astype(f32)
            for q in range(block // 128):
                at = n_b * (block // 128) + q
                decay[at, r : r + TILE, :] = a[:, q * 128 : q * 128 + 128]
                drive[at, r : r + TILE, :] = into[:, q * 128 : q * 128 + 128]
    seg = length // SEGS

    def scan(j, carry):
        h, p = carry
        s = pl.ds(j, SEGS, stride=seg)
        hs, ps = [], []
        for q in range(channels // 128):
            a = decay[q, s, :]
            hq = a * h[q] + drive[q, s, :]
            pq = a * p[q]
            drive[q, s, :] = hq
            prod[q, s, :] = pq
            hs.append(hq)
            ps.append(pq)
        return tuple(hs), tuple(ps)

    lanes = channels // 128
    zero, one = jnp.zeros((SEGS, 128), f32), jnp.ones((SEGS, 128), f32)
    lax.fori_loop(0, seg, scan, ((zero,) * lanes, (one,) * lanes), unroll=8)
    carry = [jnp.zeros((1, 128), f32)] * lanes
    pltpu.make_async_copy(weights, weights, weight_sem).wait()
    for r in range(0, length, TILE):
        rows = []
        for i in range(r, r + TILE, seg):
            s = slice(i, i + seg)
            row = []
            for q in range(lanes):
                states = drive[q, s, :] + prod[q, s, :] * carry[q]
                carry[q] = states[seg - 1 : seg, :]
                branch = jax.nn.gelu(
                    gate[s, q * 128 : q * 128 + 128].astype(f32), approximate=True
                )
                row.append((states * branch).astype(bf16))
            rows.append(jnp.concatenate(row, axis=1))
        left = jnp.concatenate(rows, axis=0)
        s = slice(r, r + TILE)
        for h in range(2):
            half = weights[h * HALF : h * HALF + HALF, :]
            part[h, s, :] = dot_turned(left, half).astype(bf16)
            pltpu.make_async_copy(part.at[h, s, :], part_out.at[h, s, :], out_sem).start()
    pltpu.make_async_copy(part, part_out, out_sem).wait()


def turned_kernel(layout, plane, *refs):
    n = len(layout)
    pos, left_in = refs[:2]
    pieces, out_ref = refs[2 : 2 + n], refs[2 + n]
    left, weights, out, sem, in_sem, out_sem = refs[3 + n :]
    tiles = out.shape[0] // TILE

    def arriving(t):
        s = pl.ds(pl.multiple_of(t * TILE, TILE), TILE)
        return pltpu.make_async_copy(left_in.at[s, :], left.at[s, :], in_sem.at[t])

    arriving(0).start()
    start_weights(pieces, layout, pos, weights, sem, plane)
    for t in range(1, tiles):
        arriving(t).start()
    pltpu.make_async_copy(weights, weights, sem).wait()

    def rows(t, _):
        arriving(t).wait()
        s = pl.ds(pl.multiple_of(t * TILE, TILE), TILE)
        out[s, :] = dot_turned(left[s, :], weights[...]).astype(bf16)
        pltpu.make_async_copy(out.at[s, :], out_ref.at[s, :], out_sem).start()
        return 0

    lax.fori_loop(0, tiles, rows, 0)
    pltpu.make_async_copy(out, out_ref, out_sem).wait()


def dot_turned(left, right):
    return lax.dot_general(left, right, (((1,), (1,)), ((), ())), preferred_element_type=f32)


def ffn_kernel(layout, *refs):
    pos, own, other, mine, theirs, gain = refs[:6]
    n = len(layout)
    pieces, (mid_out, act_out) = refs[6 : 6 + n], refs[6 + n : 8 + n]
    stream, parts, up, normed, mid, act, up_sem, in_sem, out_sem, mid_sem = refs[8 + n :]
    tiles = own.shape[0] // TILE

    def arriving(t):
        s = pl.ds(pl.multiple_of(t * TILE, TILE), TILE)
        pairs = [
            (own, stream.at[0]),
            (other, stream.at[1]),
            (mine.at[0], parts.at[0, 0]),
            (theirs.at[1], parts.at[0, 1]),
            (mine.at[1], parts.at[1, 0]),
            (theirs.at[0], parts.at[1, 1]),
        ]
        return [
            pltpu.make_async_copy(src.at[s, :], dst.at[s, :], in_sem.at[t, k])
            for k, (src, dst) in enumerate(pairs)
        ]

    def norm(t):
        s = pl.ds(pl.multiple_of(t * TILE, TILE), TILE)
        halves = []
        for h in range(2):
            v = stream[h, s, :].astype(f32) + (
                parts[h, 0, s, :].astype(f32) + parts[h, 1, s, :].astype(f32)
            )
            v = v.astype(bf16)
            mid[s, h * HALF : h * HALF + HALF] = v
            halves.append(v.astype(f32))
        a, b = halves
        ms = (jnp.sum(a * a, -1, keepdims=True) + jnp.sum(b * b, -1, keepdims=True)) / D
        r = lax.rsqrt(ms + epsilon)
        normed[s, :HALF] = (a * r * gain[:, :HALF]).astype(bf16)
        normed[s, HALF:] = (b * r * gain[:, HALF:]).astype(bf16)

    for c in arriving(0):
        c.start()
    start_weights(pieces, layout, pos, up, up_sem)
    for t in range(1, tiles):
        for c in arriving(t):
            c.start()
    for c in arriving(0):
        c.wait()
    norm(0)
    pltpu.make_async_copy(up, up, up_sem).wait()

    def product(t):
        s = pl.ds(pl.multiple_of(t * TILE, TILE), TILE)
        prod = jnp.dot(normed[s, :], up[...], preferred_element_type=f32)
        act[s, :] = jnp.square(jnp.maximum(prod, 0.0)).astype(bf16)

    def leave(t):
        s = pl.ds(pl.multiple_of(t * TILE, TILE), TILE)
        pltpu.make_async_copy(mid.at[s, :], mid_out.at[s, :], mid_sem).start()
        pltpu.make_async_copy(act.at[s, :], act_out.at[s, :], out_sem).start()

    def rows(t, _):
        for c in arriving(t + 1):
            c.wait()
        norm(t + 1)
        product(t)
        leave(t)
        return 0

    lax.fori_loop(0, tiles - 1, rows, 0)
    product(tiles - 1)
    leave(tiles - 1)
    pltpu.make_async_copy(mid, mid_out, mid_sem).wait()
    pltpu.make_async_copy(act, act_out, out_sem).wait()


def closing_kernel(pos, mid, mine_a, theirs_a, mine_b, theirs_b, gain, out_ref, *scratch):
    stream, parts, out, in_sem, out_sem = scratch
    tiles = mid.shape[0] // TILE
    near = (pos[2] + pos[3]) & 1

    def arriving(t):
        s = slice(t * TILE, (t + 1) * TILE)
        pairs = [
            (mid, stream),
            (mine_a, parts.at[near, 0]),
            (theirs_a, parts.at[near, 1]),
            (mine_b, parts.at[1 - near, 0]),
            (theirs_b, parts.at[1 - near, 1]),
        ]
        return [
            pltpu.make_async_copy(src.at[s, :], dst.at[s, :], in_sem.at[t, k])
            for k, (src, dst) in enumerate(pairs)
        ]

    for t in range(tiles):
        for c in arriving(t):
            c.start()
    for t in range(tiles):
        for c in arriving(t):
            c.wait()
        for half in range(2):
            s = slice(t * TILE + half * 128, t * TILE + half * 128 + 128)
            a, b = [
                stream[s, h * HALF : h * HALF + HALF].astype(f32)
                + (parts[h, 0, s, :].astype(f32) + parts[h, 1, s, :].astype(f32))
                for h in range(2)
            ]
            ms = (jnp.sum(a * a, -1, keepdims=True) + jnp.sum(b * b, -1, keepdims=True)) / D
            out[s, :] = (a * lax.rsqrt(ms + epsilon) * gain[...]).astype(bf16)
        s = slice(t * TILE, (t + 1) * TILE)
        pltpu.make_async_copy(out.at[s, :], out_ref.at[s, :], out_sem).start()
    pltpu.make_async_copy(out, out_ref, out_sem).wait()


def cost(flops, moved_bytes):
    return pl.CostEstimate(flops=int(flops), bytes_accessed=int(moved_bytes), transcendentals=0)


def call(kernel, out_shapes, specs, flops, scratch=(), outs=VMEM):
    return pl.pallas_call(
        kernel,
        out_shape=out_shapes,
        in_specs=specs,
        out_specs=jax.tree.map(lambda _: outs, out_shapes),
        scratch_shapes=list(scratch),
        cost_estimate=cost(flops, 8e6),
        compiler_params=pltpu.CompilerParams(vmem_limit_bytes=56 * 2**20),
    )


def flat(pieces, first_col, width, source=0):
    layout = [
        (piece[1], first_col, width, piece[2] if len(piece) > 2 else source) for piece in pieces
    ]
    return [piece[0] for piece in pieces], layout


def local(
    stream_in,
    decay_shift,
    mixer_gain,
    gate_weight,
    input_weight,
    filter_taps,
    recur_gate,
    inlet_gate,
    decay_param,
    mixer_out,
    feedforward_gain,
    up_weight,
    down_weight,
    final_gain,
):
    num_seq, length, half = stream_in.shape
    channels = gate_weight.shape[1]
    hidden = up_weight.shape[1]
    assert num_seq == 1 and half == HALF
    tp = lax.axis_index("tp")
    pos = jnp.stack(
        [lax.axis_index("x"), lax.axis_index("y"), lax.axis_index("z"), tp]
    ).astype(jnp.int32)

    def own_first(gain):
        halves = gain.reshape(2, HALF)
        return jnp.where(tp == 0, halves, halves[::-1]).reshape(1, D)

    own = stream_in.reshape(length, half)
    other = step(own, "tp", 1)

    mid_col, part = hidden // 2, channels // 2
    mixer_t, down_t = mixer_out.T, down_weight.T
    here = [(0, 0, 0, 0, 0)]
    left = jnp.concatenate([gate_weight, mixer_t[:, :part]], axis=1)[None]
    right = jnp.concatenate([mixer_t[:, part:], input_weight], axis=1)[None]
    by_x = whole_ring(left, here, "x")
    by_y = whole_ring(right, here, "y")
    pair, places = both_planes(up_weight)
    by_xy = whole_ring(*by_x, "y")
    by_yx = whole_ring(*by_y, "x")
    x_pieces = [by_xy, (step(by_xy[0], "z", 1), moved(by_xy[1], "z", 1))]
    y_pieces = [by_yx, (step(by_yx[0], "z", 3), moved(by_yx[1], "z", 1))]
    later = whole_ring(pair[:, :, :mid_col], places, "y")
    up_x = ring_pieces(*later, "x")
    later = whole_ring(pair[:, :, mid_col:], places, "x")
    up_y = ring_pieces(*later, "y")
    down_t = lax.optimization_barrier((down_t, by_x[0], by_y[0]))[0]
    plane = lax.all_gather(down_t, ("y", "x"), axis=0, tiled=False)
    down_pieces = plane_pieces(plane, 0, hidden)

    shape = jax.ShapeDtypeStruct
    whole, one_half = shape((length, D), bf16), shape((length, HALF), bf16)
    normed = call(norm_kernel, whole, [VMEM] * 3, 2e9)(own, other, own_first(mixer_gain))

    a, la = flat(x_pieces, 0, channels)
    b, lb = flat(y_pieces, channels, channels, part)
    some = shape((length, channels), bf16)
    gate, inner = call(
        functools.partial(project_kernel, la + lb),
        (some, some),
        [SMEM, VMEM] + [HBM] * len(la + lb),
        4 * length * channels * D,
        [pltpu.VMEM((D, 2 * channels), bf16), pltpu.SemaphoreType.DMA],
    )(pos, normed, *a, *b)
    scan_buffer = pltpu.VMEM((channels // 128, length, 128), f32)
    a, la = flat(x_pieces, 0, part, channels)
    b, lb = flat(y_pieces, part, part)
    partial = shape((2, length, HALF), bf16)
    mine = call(
        functools.partial(mixer_kernel, la + lb),
        partial,
        [SMEM] + [VMEM] * 7 + [HBM] * len(la + lb),
        1.2e10,
        [
            pltpu.VMEM((length + 8, channels), f32),
            scan_buffer,
            scan_buffer,
            scan_buffer,
            pltpu.VMEM((D, channels), bf16),
            pltpu.VMEM((2, length, HALF), bf16),
            pltpu.SemaphoreType.DMA,
            pltpu.SemaphoreType.DMA,
        ],
        HBM,
    )(
        pos,
        gate,
        inner,
        filter_taps,
        recur_gate,
        inlet_gate,
        (rate_scale * jax.nn.softplus(-decay_param)).reshape(1, channels),
        decay_shift.reshape(length, 1),
        *a,
        *b,
    )
    theirs = step(mine, "tp", 1)
    tiles = length // TILE

    def turned(left, pieces, plane):
        arrays, layout = flat(pieces, 0, left.shape[1])
        return call(
            functools.partial(turned_kernel, layout, plane),
            one_half,
            [SMEM, HBM] + [HBM] * len(layout),
            2 * length * left.shape[1] * HALF,
            [
                pltpu.VMEM(left.shape, bf16),
                pltpu.VMEM((HALF, left.shape[1]), bf16),
                pltpu.VMEM((length, HALF), bf16),
                pltpu.SemaphoreType.DMA,
                pltpu.SemaphoreType.DMA((tiles,)),
                pltpu.SemaphoreType.DMA,
            ],
            HBM,
        )(pos, left, *arrays)

    a, la = flat(up_x, 0, mid_col)
    b, lb = flat(up_y, mid_col, mid_col)
    mid, activated = call(
        functools.partial(ffn_kernel, la + lb),
        (whole, shape((length, hidden), bf16)),
        [SMEM] + [HBM] * 4 + [VMEM] + [HBM] * len(la + lb),
        2 * length * hidden * D,
        [
            pltpu.VMEM((2, length, HALF), bf16),
            pltpu.VMEM((2, 2, length, HALF), bf16),
            pltpu.VMEM((D, hidden), bf16),
            pltpu.VMEM((length, D), bf16),
            pltpu.VMEM((length, D), bf16),
            pltpu.VMEM((length, hidden), bf16),
            pltpu.SemaphoreType.DMA,
            pltpu.SemaphoreType.DMA((tiles, 6)),
            pltpu.SemaphoreType.DMA,
            pltpu.SemaphoreType.DMA,
        ],
        HBM,
    )(pos, own, other, mine, theirs, own_first(feedforward_gain), *a, *b)
    mine_c = turned(activated, down_pieces[:1], 0)
    theirs_c = step(mine_c, "tp", 1)
    mine_d = turned(activated, down_pieces[1:], 1)
    theirs_d = step(mine_d, "tp", 1)
    out = call(
        closing_kernel,
        one_half,
        [SMEM] + [HBM] * 5 + [VMEM],
        2e9,
        [
            pltpu.VMEM((length, D), bf16),
            pltpu.VMEM((2, 2, length, HALF), bf16),
            pltpu.VMEM((length, HALF), bf16),
            pltpu.SemaphoreType.DMA((tiles, 5)),
            pltpu.SemaphoreType.DMA,
        ],
        HBM,
    )(pos, mid, mine_c, theirs_c, mine_d, theirs_d, final_gain.reshape(1, HALF))
    return out.reshape(num_seq, length, half)


def solution(mesh):
    grid = Mesh(mesh.devices.reshape(2, 2, 4, 4, 2), ("rep", "z", "y", "x", "tp"))
    fs = ("z", "y", "x")
    seqs = ("rep",) + fs
    return jax.shard_map(
        local,
        mesh=grid,
        in_specs=(
            P(seqs, None, "tp"),
            P(seqs, None),
            P(),
            P(fs, "tp"),
            P(fs, "tp"),
            P(None, "tp"),
            P("tp", None, None),
            P("tp", None, None),
            P("tp"),
            P("tp", fs),
            P(),
            P(fs, "tp"),
            P("tp", fs),
            P("tp"),
        ),
        out_specs=P(seqs, None, "tp"),
        check_vma=False,
    )
```

```python
import functools

import jax
import jax.numpy as jnp
from jax import lax
from jax.experimental import pallas as pl
from jax.experimental.pallas import tpu as pltpu
from jax.sharding import Mesh, PartitionSpec as P

D = 2048
HALF = 1024
ROWS = 64
TILE = 256
SEGS = 8

epsilon = 1e-06
rate_scale = 8.0


f32, bf16 = jnp.float32, jnp.bfloat16
VMEM = pl.BlockSpec(memory_space=pltpu.VMEM)
HBM = pl.BlockSpec(memory_space=pltpu.HBM)
SMEM = pl.BlockSpec(memory_space=pltpu.SMEM)


def step(v, axis, shift):
    size = 2 if axis == "tp" else 4
    over = ("rep", "z") if axis == "z" else axis
    return lax.ppermute(v, over, [(i, (i + shift) % size) for i in range(size)])


def moved(places, axis, by):
    at = "xyz".index(axis)
    return [p[:at] + (p[at] + by,) + p[at + 1 :] for p in places]


def both_planes(shard):
    half = shard.shape[0] // 2
    lower = step(shard[:half], "z", 1)
    upper = step(shard[half:], "z", 3)
    pair = jnp.stack([shard, jnp.concatenate([lower, upper], axis=0)])
    return pair, [(0, 0, 0, 0, 0), (0, 0, 1, 0, 0)]


def ring_pieces(v, places, axis):
    far = step(v, axis, 2)
    left = step(v, axis, 1)
    right = step(v, axis, 3)
    return [
        (v, places),
        (left, moved(places, axis, -1)),
        (right, moved(places, axis, 1)),
        (far, moved(places, axis, 2)),
    ]


def whole_ring(v, places, axis):
    pieces = ring_pieces(v, places, axis)
    return jnp.concatenate([p for p, _ in pieces], axis=0), sum((q for _, q in pieces), [])


def plane_pieces(own, first, width):
    half = own.shape[0] // 2
    places = [(i % 4, i // 4, 0, 1, 0) for i in range(2 * half)]
    lower = step(own[:half, :, first : first + width], "z", 1)
    upper = step(own[half:, :, first : first + width], "z", 3)
    far = moved(places, "z", 1)
    return [(own, places, first), (lower, far[:half]), (upper, far[half:])]


def start_weights(refs, layout, pos, target, sem, plane=None):
    x, y, z, tp = pos[0], pos[1], pos[2], pos[3]
    for ref, (places, first_col, width, source_col) in zip(refs, layout):
        cols, source = pl.ds(first_col, width), pl.ds(source_col, width)
        for b, (px, py, pz, absolute, first_row) in enumerate(places):
            line = (py * 4 + px) if absolute else ((y + py) & 3) * 4 + ((x + px) & 3)
            at = line * ROWS + first_row
            if plane is None:
                at = ((z + pz + tp) & 1) * HALF + at
            elif pz != plane:
                continue
            at = at if isinstance(at, int) else pl.multiple_of(at, 16)
            pltpu.make_async_copy(
                ref.at[b, :, source], target.at[pl.ds(at, ref.shape[1]), cols], sem
            ).start()


def norm_kernel(own, other, gain, normed):
    def rows(i, _):
        s = pl.ds(pl.multiple_of(i * TILE, TILE), TILE)
        a, b = own[s, :].astype(f32), other[s, :].astype(f32)
        ms = (jnp.sum(a * a, -1, keepdims=True) + jnp.sum(b * b, -1, keepdims=True)) / D
        r = lax.rsqrt(ms + epsilon)
        normed[s, :HALF] = (a * r * gain[:, :HALF]).astype(bf16)
        normed[s, HALF:] = (b * r * gain[:, HALF:]).astype(bf16)
        return 0

    lax.fori_loop(0, own.shape[0] // TILE, rows, 0)


def mixer_kernel(in_layout, out_layout, *refs):
    n, m = len(in_layout), len(out_layout)
    pos, normed, taps, recur_gate, inlet_gate, rate, shift = refs[:7]
    in_pieces, out_pieces, part_out = refs[7 : 7 + n], refs[7 + n : 7 + n + m], refs[7 + n + m]
    entry, gate, padded, decay, drive, prod, weights, part = refs[8 + n + m : -3]
    in_sem, weight_sem, out_sem = refs[-3:]
    length, channels = gate.shape
    start_weights(in_pieces, in_layout, pos, entry, in_sem)
    start_weights(out_pieces, out_layout, pos, weights, weight_sem)
    padded[:8, :] = jnp.zeros((8, channels), f32)
    blocks, block = recur_gate.shape[0], recur_gate.shape[1]
    pltpu.make_async_copy(entry, entry, in_sem).wait()
    for r in range(0, length, TILE):
        both = jnp.dot(normed[r : r + TILE, :], entry[...], preferred_element_type=f32)
        both = both.astype(bf16)
        gate[r : r + TILE, :] = both[:, :channels]
        padded[8 + r : 8 + r + TILE, :] = both[:, channels:].astype(f32)
        acc = padded[r + 5 : r + 5 + TILE, :] * taps[0:1, :]
        for k in range(1, 4):
            acc = acc + padded[r + 5 + k : r + 5 + k + TILE, :] * taps[k : k + 1, :]
        filt = acc.astype(bf16)
        for n_b in range(blocks):
            cols = slice(n_b * block, (n_b + 1) * block)
            fb = filt[:, cols]
            recur = jax.nn.sigmoid(jnp.dot(fb, recur_gate[n_b], preferred_element_type=f32))
            inlet = jax.nn.sigmoid(jnp.dot(fb, inlet_gate[n_b], preferred_element_type=f32))
            log_decay = shift[r : r + TILE, :] - recur * rate[:, cols]
            a = jnp.exp(log_decay)
            t = 2.0 * log_decay
            series = -t * (
                1.0
                + t
                * (
                    1.0 / 2
                    + t
                    * (1.0 / 6 + t * (1.0 / 24 + t * (1.0 / 120 + t * (1.0 / 720 + t / 5040))))
                )
            )
            gone = jnp.where(t > -0.4, series, 1.0 - a * a)
            into = jnp.sqrt(gone) * inlet * fb.astype(f32)
            for q in range(block // 128):
                at = n_b * (block // 128) + q
                decay[at, r : r + TILE, :] = a[:, q * 128 : q * 128 + 128]
                drive[at, r : r + TILE, :] = into[:, q * 128 : q * 128 + 128]
    seg = length // SEGS

    def scan(j, carry):
        h, p = carry
        s = pl.ds(j, SEGS, stride=seg)
        hs, ps = [], []
        for q in range(channels // 128):
            a = decay[q, s, :]
            hq = a * h[q] + drive[q, s, :]
            pq = a * p[q]
            drive[q, s, :] = hq
            prod[q, s, :] = pq
            hs.append(hq)
            ps.append(pq)
        return tuple(hs), tuple(ps)

    lanes = channels // 128
    zero, one = jnp.zeros((SEGS, 128), f32), jnp.ones((SEGS, 128), f32)
    lax.fori_loop(0, seg, scan, ((zero,) * lanes, (one,) * lanes), unroll=8)
    carry = [jnp.zeros((1, 128), f32)] * lanes
    pltpu.make_async_copy(weights, weights, weight_sem).wait()
    for r in range(0, length, TILE):
        rows = []
        for i in range(r, r + TILE, seg):
            s = slice(i, i + seg)
            row = []
            for q in range(lanes):
                states = drive[q, s, :] + prod[q, s, :] * carry[q]
                carry[q] = states[seg - 1 : seg, :]
                branch = jax.nn.gelu(
                    gate[s, q * 128 : q * 128 + 128].astype(f32), approximate=True
                )
                row.append((states * branch).astype(bf16))
            rows.append(jnp.concatenate(row, axis=1))
        left = jnp.concatenate(rows, axis=0)
        s = slice(r, r + TILE)
        for h in range(2):
            half = weights[h * HALF : h * HALF + HALF, :]
            part[h, s, :] = dot_turned(left, half).astype(bf16)
            pltpu.make_async_copy(part.at[h, s, :], part_out.at[h, s, :], out_sem).start()
    pltpu.make_async_copy(part, part_out, out_sem).wait()


def turned_kernel(layout, plane, *refs):
    n = len(layout)
    pos, left_in = refs[:2]
    pieces, out_ref = refs[2 : 2 + n], refs[2 + n]
    left, weights, out, sem, in_sem, out_sem = refs[3 + n :]
    tiles = out.shape[0] // TILE

    def arriving(t):
        s = pl.ds(pl.multiple_of(t * TILE, TILE), TILE)
        return pltpu.make_async_copy(left_in.at[s, :], left.at[s, :], in_sem.at[t])

    arriving(0).start()
    start_weights(pieces, layout, pos, weights, sem, plane)
    for t in range(1, tiles):
        arriving(t).start()
    pltpu.make_async_copy(weights, weights, sem).wait()

    def rows(t, _):
        arriving(t).wait()
        s = pl.ds(pl.multiple_of(t * TILE, TILE), TILE)
        out[s, :] = dot_turned(left[s, :], weights[...]).astype(bf16)
        pltpu.make_async_copy(out.at[s, :], out_ref.at[s, :], out_sem).start()
        return 0

    lax.fori_loop(0, tiles, rows, 0)
    pltpu.make_async_copy(out, out_ref, out_sem).wait()


def dot_turned(left, right):
    return lax.dot_general(left, right, (((1,), (1,)), ((), ())), preferred_element_type=f32)


def ffn_kernel(layout, down_layout, *refs):
    pos, own, other, mine, theirs, gain = refs[:6]
    n, m = len(layout), len(down_layout)
    pieces, down_pieces = refs[6 : 6 + n], refs[6 + n : 6 + n + m]
    mid_out, act_out, part_out = refs[6 + n + m : 9 + n + m]
    stream, parts, up, down, mid, act, part = refs[9 + n + m : 16 + n + m]
    tiles = own.shape[0] // TILE
    normed = refs[16 + n + m : 16 + n + m + tiles]
    up_sem, down_sem, in_sem, act_sem, mid_sem, part_sem = refs[16 + n + m + tiles :]

    def arriving(t):
        s = slice(t * TILE, (t + 1) * TILE)
        pairs = [
            (own, stream.at[0]),
            (other, stream.at[1]),
            (mine.at[0], parts.at[0, 0]),
            (theirs.at[1], parts.at[0, 1]),
            (mine.at[1], parts.at[1, 0]),
            (theirs.at[0], parts.at[1, 1]),
        ]
        return [
            pltpu.make_async_copy(src.at[s, :], dst.at[s, :], in_sem.at[t, k])
            for k, (src, dst) in enumerate(pairs)
        ]

    def norm(t):
        for c in arriving(t):
            c.wait()
        s = slice(t * TILE, (t + 1) * TILE)
        halves = []
        for h in range(2):
            v = stream[h, s, :].astype(f32) + (
                parts[h, 0, s, :].astype(f32) + parts[h, 1, s, :].astype(f32)
            )
            v = v.astype(bf16)
            mid[s, h * HALF : h * HALF + HALF] = v
            halves.append(v.astype(f32))
        a, b = halves
        ms = (jnp.sum(a * a, -1, keepdims=True) + jnp.sum(b * b, -1, keepdims=True)) / D
        r = lax.rsqrt(ms + epsilon)
        normed[t][:, :HALF] = (a * r * gain[:, :HALF]).astype(bf16)
        normed[t][:, HALF:] = (b * r * gain[:, HALF:]).astype(bf16)
        pltpu.make_async_copy(mid.at[s, :], mid_out.at[s, :], mid_sem).start()

    for c in arriving(0):
        c.start()
    start_weights(pieces, layout, pos, up, up_sem)
    for c in arriving(1):
        c.start()
    start_weights(down_pieces, down_layout, pos, down, down_sem, 0)
    for t in range(2, tiles):
        for c in arriving(t):
            c.start()
    norm(0)
    pltpu.make_async_copy(up, up, up_sem).wait()
    for t in range(tiles):
        s = slice(t * TILE, (t + 1) * TILE)
        if t + 1 < tiles:
            norm(t + 1)
        prod = jnp.dot(normed[t][...], up[...], preferred_element_type=f32)
        left = jnp.square(jnp.maximum(prod, 0.0)).astype(bf16)
        act[s, :] = left
        pltpu.make_async_copy(act.at[s, :], act_out.at[s, :], act_sem).start()
        if t == 0:
            pltpu.make_async_copy(down, down, down_sem).wait()
        part[s, :] = dot_turned(left, down[...]).astype(bf16)
        pltpu.make_async_copy(part.at[s, :], part_out.at[s, :], part_sem).start()
    pltpu.make_async_copy(mid, mid_out, mid_sem).wait()
    pltpu.make_async_copy(act, act_out, act_sem).wait()
    pltpu.make_async_copy(part, part_out, part_sem).wait()


def closing_kernel(pos, mid, mine_a, theirs_a, mine_b, theirs_b, gain, out_ref, *scratch):
    stream, parts, out, in_sem, out_sem = scratch
    tiles = mid.shape[0] // TILE
    near = (pos[2] + pos[3]) & 1

    def arriving(t):
        s = slice(t * TILE, (t + 1) * TILE)
        pairs = [
            (mid.at[s, :HALF], stream.at[near, s, :]),
            (mid.at[s, HALF:], stream.at[1 - near, s, :]),
            (mine_a.at[s, :], parts.at[0, s, :]),
            (theirs_a.at[s, :], parts.at[1, s, :]),
            (mine_b.at[s, :], parts.at[2, s, :]),
        ]
        return [
            pltpu.make_async_copy(src, dst, in_sem.at[t, k]) for k, (src, dst) in enumerate(pairs)
        ]

    for t in range(tiles):
        for c in arriving(t):
            c.start()
    for t in range(tiles):
        for c in arriving(t):
            c.wait()
        for half in range(2):
            s = slice(t * TILE + half * 128, t * TILE + half * 128 + 128)
            a = stream[0, s, :].astype(f32) + (
                parts[0, s, :].astype(f32) + parts[1, s, :].astype(f32)
            )
            b = stream[1, s, :].astype(f32) + (
                parts[2, s, :].astype(f32) + theirs_b[s, :].astype(f32)
            )
            ms = (jnp.sum(a * a, -1, keepdims=True) + jnp.sum(b * b, -1, keepdims=True)) / D
            mine = jnp.where(near == 0, a, b)
            out[s, :] = (mine * lax.rsqrt(ms + epsilon) * gain[...]).astype(bf16)
        s = slice(t * TILE, (t + 1) * TILE)
        pltpu.make_async_copy(out.at[s, :], out_ref.at[s, :], out_sem).start()
    pltpu.make_async_copy(out, out_ref, out_sem).wait()


def cost(flops, moved_bytes):
    return pl.CostEstimate(flops=int(flops), bytes_accessed=int(moved_bytes), transcendentals=0)


def call(kernel, out_shapes, specs, flops, scratch=(), outs=VMEM, room=56):
    return pl.pallas_call(
        kernel,
        out_shape=out_shapes,
        in_specs=specs,
        out_specs=jax.tree.map(lambda _: outs, out_shapes),
        scratch_shapes=list(scratch),
        cost_estimate=cost(flops, 8e6),
        compiler_params=pltpu.CompilerParams(vmem_limit_bytes=room * 2**20),
    )


def flat(pieces, first_col, width, source=0):
    layout = [
        (piece[1], first_col, width, piece[2] if len(piece) > 2 else source) for piece in pieces
    ]
    return [piece[0] for piece in pieces], layout


def local(
    stream_in,
    decay_shift,
    mixer_gain,
    gate_weight,
    input_weight,
    filter_taps,
    recur_gate,
    inlet_gate,
    decay_param,
    mixer_out,
    feedforward_gain,
    up_weight,
    down_weight,
    final_gain,
):
    num_seq, length, half = stream_in.shape
    channels = gate_weight.shape[1]
    hidden = up_weight.shape[1]
    assert num_seq == 1 and half == HALF
    tp = lax.axis_index("tp")
    pos = jnp.stack(
        [lax.axis_index("x"), lax.axis_index("y"), lax.axis_index("z"), tp]
    ).astype(jnp.int32)

    def own_first(gain):
        halves = gain.reshape(2, HALF)
        return jnp.where(tp == 0, halves, halves[::-1]).reshape(1, D)

    own = stream_in.reshape(length, half)
    other = step(own, "tp", 1)

    mid_col, part = hidden // 2, channels // 2
    mixer_t, down_t = mixer_out.T, down_weight.T
    here = [(0, 0, 0, 0, 0)]
    left = jnp.concatenate([gate_weight, mixer_t[:, :part]], axis=1)[None]
    right = jnp.concatenate([mixer_t[:, part:], input_weight], axis=1)[None]
    by_x = whole_ring(left, here, "x")
    by_y = whole_ring(right, here, "y")
    pair, places = both_planes(up_weight)
    by_xy = whole_ring(*by_x, "y")
    by_yx = whole_ring(*by_y, "x")
    x_pieces = [by_xy, (step(by_xy[0], "z", 1), moved(by_xy[1], "z", 1))]
    y_pieces = [by_yx, (step(by_yx[0], "z", 3), moved(by_yx[1], "z", 1))]
    later = whole_ring(pair[:, :, :mid_col], places, "y")
    up_x = ring_pieces(*later, "x")
    later = whole_ring(pair[:, :, mid_col:], places, "x")
    up_y = ring_pieces(*later, "y")
    plane = lax.all_gather(down_t, ("y", "x"), axis=0, tiled=False)
    down_pieces = plane_pieces(plane, 0, hidden)

    shape = jax.ShapeDtypeStruct
    whole, one_half = shape((length, D), bf16), shape((length, HALF), bf16)
    normed = call(norm_kernel, whole, [VMEM] * 3, 2e9, room=24)(own, other, own_first(mixer_gain))

    scan_buffer = pltpu.VMEM((channels // 128, length, 128), f32)
    a, la = flat(x_pieces, 0, channels)
    b, lb = flat(y_pieces, channels, channels, part)
    c, lc = flat(x_pieces, 0, part, channels)
    d, ld = flat(y_pieces, part, part)
    partial = shape((2, length, HALF), bf16)
    mine = call(
        functools.partial(mixer_kernel, la + lb, lc + ld),
        partial,
        [SMEM] + [VMEM] * 6 + [HBM] * len(la + lb + lc + ld),
        1.2e10,
        [
            pltpu.VMEM((D, 2 * channels), bf16),
            pltpu.VMEM((length, channels), bf16),
            pltpu.VMEM((length + 8, channels), f32),
            scan_buffer,
            scan_buffer,
            scan_buffer,
            pltpu.VMEM((D, channels), bf16),
            pltpu.VMEM((2, length, HALF), bf16),
            pltpu.SemaphoreType.DMA,
            pltpu.SemaphoreType.DMA,
            pltpu.SemaphoreType.DMA,
        ],
        HBM,
    )(
        pos,
        normed,
        filter_taps,
        recur_gate,
        inlet_gate,
        (rate_scale * jax.nn.softplus(-decay_param)).reshape(1, channels),
        decay_shift.reshape(length, 1),
        *a,
        *b,
        *c,
        *d,
    )
    theirs = step(mine, "tp", 1)
    tiles = length // TILE

    def turned(left, pieces, plane):
        arrays, layout = flat(pieces, 0, left.shape[1])
        return call(
            functools.partial(turned_kernel, layout, plane),
            one_half,
            [SMEM, HBM] + [HBM] * len(layout),
            2 * length * left.shape[1] * HALF,
            [
                pltpu.VMEM(left.shape, bf16),
                pltpu.VMEM((HALF, left.shape[1]), bf16),
                pltpu.VMEM((length, HALF), bf16),
                pltpu.SemaphoreType.DMA,
                pltpu.SemaphoreType.DMA((tiles,)),
                pltpu.SemaphoreType.DMA,
            ],
            HBM,
        )(pos, left, *arrays)

    a, la = flat(up_x, 0, mid_col)
    b, lb = flat(up_y, mid_col, mid_col)
    c, lc = flat(down_pieces[:1], 0, hidden)
    mid, activated, mine_c = call(
        functools.partial(ffn_kernel, la + lb, lc),
        (whole, shape((length, hidden), bf16), one_half),
        [SMEM] + [HBM] * 4 + [VMEM] + [HBM] * len(la + lb + lc),
        3 * length * hidden * D,
        [
            pltpu.VMEM((2, length, HALF), bf16),
            pltpu.VMEM((2, 2, length, HALF), bf16),
            pltpu.VMEM((D, hidden), bf16),
            pltpu.VMEM((HALF, hidden), bf16),
            pltpu.VMEM((length, D), bf16),
            pltpu.VMEM((length, hidden), bf16),
            pltpu.VMEM((length, HALF), bf16),
        ]
        + [pltpu.VMEM((TILE, D), bf16)] * tiles
        + [
            pltpu.SemaphoreType.DMA,
            pltpu.SemaphoreType.DMA,
            pltpu.SemaphoreType.DMA((tiles, 6)),
            pltpu.SemaphoreType.DMA,
            pltpu.SemaphoreType.DMA,
            pltpu.SemaphoreType.DMA,
        ],
        HBM,
    )(pos, own, other, mine, theirs, own_first(feedforward_gain), *a, *b, *c)
    theirs_c = step(mine_c, "tp", 1)
    mine_d = turned(activated, down_pieces[1:], 1)
    theirs_d = step(mine_d, "tp", 1)
    out = call(
        closing_kernel,
        one_half,
        [SMEM] + [HBM] * 4 + [VMEM] * 2,
        2e9,
        [
            pltpu.VMEM((2, length, HALF), bf16),
            pltpu.VMEM((3, length, HALF), bf16),
            pltpu.VMEM((length, HALF), bf16),
            pltpu.SemaphoreType.DMA((tiles, 5)),
            pltpu.SemaphoreType.DMA,
        ],
        HBM,
        24,
    )(pos, mid, mine_c, theirs_c, mine_d, theirs_d, final_gain.reshape(1, HALF))
    return out.reshape(num_seq, length, half)


def solution(mesh):
    grid = Mesh(mesh.devices.reshape(2, 2, 4, 4, 2), ("rep", "z", "y", "x", "tp"))
    fs = ("z", "y", "x")
    seqs = ("rep",) + fs
    return jax.shard_map(
        local,
        mesh=grid,
        in_specs=(
            P(seqs, None, "tp"),
            P(seqs, None),
            P(),
            P(fs, "tp"),
            P(fs, "tp"),
            P(None, "tp"),
            P("tp", None, None),
            P("tp", None, None),
            P("tp"),
            P("tp", fs),
            P(),
            P(fs, "tp"),
            P("tp", fs),
            P("tp"),
        ),
        out_specs=P(seqs, None, "tp"),
        check_vma=False,
    )
```

```python
import functools

import jax
import jax.numpy as jnp
from jax import lax
from jax.experimental import pallas as pl
from jax.experimental.pallas import tpu as pltpu
from jax.sharding import Mesh, PartitionSpec as P

D = 2048
HALF = 1024
ROWS = 64
TILE = 256
SEGS = 8

epsilon = 1e-06
rate_scale = 8.0


f32, bf16 = jnp.float32, jnp.bfloat16
VMEM = pl.BlockSpec(memory_space=pltpu.VMEM)
HBM = pl.BlockSpec(memory_space=pltpu.HBM)
SMEM = pl.BlockSpec(memory_space=pltpu.SMEM)


def step(v, axis, shift):
    size = 2 if axis == "tp" else 4
    over = ("rep", "z") if axis == "z" else axis
    return lax.ppermute(v, over, [(i, (i + shift) % size) for i in range(size)])


def moved(places, axis, by):
    at = "xyz".index(axis)
    return [p[:at] + (p[at] + by,) + p[at + 1 :] for p in places]


def both_planes(shard):
    half = shard.shape[0] // 2
    lower = step(shard[:half], "z", 1)
    upper = step(shard[half:], "z", 3)
    pair = jnp.stack([shard, jnp.concatenate([lower, upper], axis=0)])
    return pair, [(0, 0, 0, 0, 0), (0, 0, 1, 0, 0)]


def ring_pieces(v, places, axis):
    far = step(v, axis, 2)
    left = step(v, axis, 1)
    right = step(v, axis, 3)
    return [
        (v, places),
        (left, moved(places, axis, -1)),
        (right, moved(places, axis, 1)),
        (far, moved(places, axis, 2)),
    ]


def whole_ring(v, places, axis):
    pieces = ring_pieces(v, places, axis)
    return jnp.concatenate([p for p, _ in pieces], axis=0), sum((q for _, q in pieces), [])


def start_weights(refs, layout, pos, target, sem, plane=None):
    x, y, z, tp = pos[0], pos[1], pos[2], pos[3]
    for ref, (places, first_col, width, source_col) in zip(refs, layout):
        cols, source = pl.ds(first_col, width), pl.ds(source_col, width)
        for b, (px, py, pz, absolute, first_row) in enumerate(places):
            line = (py * 4 + px) if absolute else ((y + py) & 3) * 4 + ((x + px) & 3)
            at = line * ROWS + first_row
            if plane is None:
                at = ((z + pz + tp) & 1) * HALF + at
            elif pz != plane:
                continue
            at = at if isinstance(at, int) else pl.multiple_of(at, 16)
            pltpu.make_async_copy(
                ref.at[b, :, source], target.at[pl.ds(at, ref.shape[1]), cols], sem
            ).start()


def sort_kernel(*refs):
    pieces, (down, up), sem = refs[:4], refs[4:6], refs[6]
    copies = []
    for k, piece in enumerate(pieces):
        copies.append((piece.at[4:6], up.at[2 * k : 2 * k + 2], sem.at[2 * k]))
        copies.append((piece.at[0:4], down.at[4 * k : 4 * k + 4], sem.at[2 * k + 1]))
    copies = [pltpu.make_async_copy(*c) for c in copies]
    for c in copies:
        c.start()
    for c in copies:
        c.wait()


def norm_kernel(own, other, gain, normed):
    def rows(i, _):
        s = pl.ds(pl.multiple_of(i * TILE, TILE), TILE)
        a, b = own[s, :].astype(f32), other[s, :].astype(f32)
        ms = (jnp.sum(a * a, -1, keepdims=True) + jnp.sum(b * b, -1, keepdims=True)) / D
        r = lax.rsqrt(ms + epsilon)
        normed[s, :HALF] = (a * r * gain[:, :HALF]).astype(bf16)
        normed[s, HALF:] = (b * r * gain[:, HALF:]).astype(bf16)
        return 0

    lax.fori_loop(0, own.shape[0] // TILE, rows, 0)


def mixer_kernel(in_layout, out_layout, *refs):
    n, m = len(in_layout), len(out_layout)
    pos, normed, taps, recur_gate, inlet_gate, rate, shift = refs[:7]
    in_pieces, out_pieces, part_out = refs[7 : 7 + n], refs[7 + n : 7 + n + m], refs[7 + n + m]
    entry, gate, padded, decay, drive, prod, weights, part = refs[8 + n + m : -3]
    in_sem, weight_sem, out_sem = refs[-3:]
    length, channels = gate.shape
    start_weights(in_pieces, in_layout, pos, entry, in_sem)
    start_weights(out_pieces, out_layout, pos, weights, weight_sem)
    padded[:8, :] = jnp.zeros((8, channels), f32)
    blocks, block = recur_gate.shape[0], recur_gate.shape[1]
    pltpu.make_async_copy(entry, entry, in_sem).wait()

    def enter(i, _):
        s = pl.ds(pl.multiple_of(i * TILE, TILE), TILE)
        both = jnp.dot(normed[s, :], entry[...], preferred_element_type=f32).astype(bf16)
        gate[s, :] = both[:, :channels]
        padded[pl.ds(pl.multiple_of(8 + i * TILE, 8), TILE), :] = both[:, channels:].astype(f32)
        window = padded[pl.ds(pl.multiple_of(i * TILE, TILE), TILE + 8), :]
        acc = window[5 : 5 + TILE, :] * taps[0:1, :]
        for k in range(1, 4):
            acc = acc + window[5 + k : 5 + k + TILE, :] * taps[k : k + 1, :]
        filt = acc.astype(bf16)
        for n_b in range(blocks):
            cols = slice(n_b * block, (n_b + 1) * block)
            fb = filt[:, cols]
            recur = jax.nn.sigmoid(jnp.dot(fb, recur_gate[n_b], preferred_element_type=f32))
            inlet = jax.nn.sigmoid(jnp.dot(fb, inlet_gate[n_b], preferred_element_type=f32))
            log_decay = shift[s, :] - recur * rate[:, cols]
            a = jnp.exp(log_decay)
            t = 2.0 * log_decay
            series = 1.0 / 120 + t * (1.0 / 720 + t / 5040)
            series = 1.0 / 2 + t * (1.0 / 6 + t * (1.0 / 24 + t * series))
            series = -t * (1.0 + t * series)
            gone = jnp.where(t > -0.4, series, 1.0 - a * a)
            into = jnp.sqrt(gone) * inlet * fb.astype(f32)
            for q in range(block // 128):
                at = n_b * (block // 128) + q
                decay[at, s, :] = a[:, q * 128 : q * 128 + 128]
                drive[at, s, :] = into[:, q * 128 : q * 128 + 128]
        return 0

    lax.fori_loop(0, length // TILE, enter, 0)
    seg = length // SEGS

    def scan(j, carry):
        h, p = carry
        s = pl.ds(j, SEGS, stride=seg)
        hs, ps = [], []
        for q in range(channels // 128):
            a = decay[q, s, :]
            hq = a * h[q] + drive[q, s, :]
            pq = a * p[q]
            drive[q, s, :] = hq
            prod[q, s, :] = pq
            hs.append(hq)
            ps.append(pq)
        return tuple(hs), tuple(ps)

    lanes = channels // 128
    zero, one = jnp.zeros((SEGS, 128), f32), jnp.ones((SEGS, 128), f32)
    lax.fori_loop(0, seg, scan, ((zero,) * lanes, (one,) * lanes), unroll=8)
    pltpu.make_async_copy(weights, weights, weight_sem).wait()

    def leave(r, carry):
        carry, rows = list(carry), []
        for i in range(TILE // seg):
            s = pl.ds(pl.multiple_of(r * TILE + i * seg, seg), seg)
            row = []
            for q in range(lanes):
                states = drive[q, s, :] + prod[q, s, :] * carry[q]
                carry[q] = states[seg - 1 : seg, :]
                branch = jax.nn.gelu(
                    gate[s, q * 128 : q * 128 + 128].astype(f32), approximate=True
                )
                row.append((states * branch).astype(bf16))
            rows.append(jnp.concatenate(row, axis=1))
        left = jnp.concatenate(rows, axis=0)
        s = pl.ds(pl.multiple_of(r * TILE, TILE), TILE)
        for h in range(2):
            half = weights[h * HALF : h * HALF + HALF, :]
            part[h, s, :] = dot_turned(left, half).astype(bf16)
            pltpu.make_async_copy(part.at[h, s, :], part_out.at[h, s, :], out_sem).start()
        return tuple(carry)

    lax.fori_loop(0, length // TILE, leave, (jnp.zeros((1, 128), f32),) * lanes)
    pltpu.make_async_copy(part, part_out, out_sem).wait()


def turned_kernel(layout, plane, *refs):
    n = len(layout)
    pos, left_in = refs[:2]
    pieces, out = refs[2 : 2 + n], refs[2 + n]
    left, weights, sem, in_sem = refs[3 + n :]
    tiles = out.shape[0] // TILE

    def arriving(t):
        s = pl.ds(pl.multiple_of(t * TILE, TILE), TILE)
        return pltpu.make_async_copy(left_in.at[s, :], left.at[s, :], in_sem.at[t])

    arriving(0).start()
    start_weights(pieces, layout, pos, weights, sem, plane)
    for t in range(1, tiles):
        arriving(t).start()
    pltpu.make_async_copy(weights, weights, sem).wait()

    def rows(t, _):
        arriving(t).wait()
        s = pl.ds(pl.multiple_of(t * TILE, TILE), TILE)
        out[s, :] = dot_turned(left[s, :], weights[...]).astype(bf16)
        return 0

    lax.fori_loop(0, tiles, rows, 0)


def dot_turned(left, right):
    return lax.dot_general(left, right, (((1,), (1,)), ((), ())), preferred_element_type=f32)


def ffn_kernel(layout, down_layout, *refs):
    pos, own, other, mine, theirs, gain = refs[:6]
    n, m = len(layout), len(down_layout)
    pieces, down_pieces = refs[6 : 6 + n], refs[6 + n : 6 + n + m]
    mid_out, act_out, part_out = refs[6 + n + m : 9 + n + m]
    stream, parts, up, down, normed, mid, act, part = refs[9 + n + m : 17 + n + m]
    up_sem, down_sem, in_sem, act_sem, mid_sem, part_sem = refs[17 + n + m :]
    tiles = own.shape[0] // TILE

    def arriving(t):
        s = pl.ds(pl.multiple_of(t * TILE, TILE), TILE)
        pairs = [
            (own, stream.at[0]),
            (other, stream.at[1]),
            (mine.at[0], parts.at[0, 0]),
            (theirs.at[1], parts.at[0, 1]),
            (mine.at[1], parts.at[1, 0]),
            (theirs.at[0], parts.at[1, 1]),
        ]
        return [
            pltpu.make_async_copy(src.at[s, :], dst.at[s, :], in_sem.at[t, k])
            for k, (src, dst) in enumerate(pairs)
        ]

    for c in arriving(0):
        c.start()
    start_weights(pieces, layout, pos, up, up_sem)
    for c in arriving(1):
        c.start()
    start_weights(down_pieces, down_layout, pos, down, down_sem, 0)
    for t in range(2, tiles):
        for c in arriving(t):
            c.start()

    def rows(t, _):
        for c in arriving(t):
            c.wait()
        s = pl.ds(pl.multiple_of(t * TILE, TILE), TILE)
        halves = []
        for h in range(2):
            v = stream[h, s, :].astype(f32) + (
                parts[h, 0, s, :].astype(f32) + parts[h, 1, s, :].astype(f32)
            )
            v = v.astype(bf16)
            mid[s, h * HALF : h * HALF + HALF] = v
            halves.append(v.astype(f32))
        a, b = halves
        ms = (jnp.sum(a * a, -1, keepdims=True) + jnp.sum(b * b, -1, keepdims=True)) / D
        r = lax.rsqrt(ms + epsilon)
        normed[:, :HALF] = (a * r * gain[:, :HALF]).astype(bf16)
        normed[:, HALF:] = (b * r * gain[:, HALF:]).astype(bf16)
        pltpu.make_async_copy(mid.at[s, :], mid_out.at[s, :], mid_sem).start()

        @pl.when(t == 0)
        def _():
            pltpu.make_async_copy(up, up, up_sem).wait()
            pltpu.make_async_copy(down, down, down_sem).wait()

        prod = jnp.dot(normed[...], up[...], preferred_element_type=f32)
        left = jnp.square(jnp.maximum(prod, 0.0)).astype(bf16)
        act[s, :] = left
        pltpu.make_async_copy(act.at[s, :], act_out.at[s, :], act_sem).start()
        part[s, :] = dot_turned(left, down[...]).astype(bf16)
        pltpu.make_async_copy(part.at[s, :], part_out.at[s, :], part_sem).start()
        return 0

    lax.fori_loop(0, tiles, rows, 0)
    pltpu.make_async_copy(mid, mid_out, mid_sem).wait()
    pltpu.make_async_copy(act, act_out, act_sem).wait()
    pltpu.make_async_copy(part, part_out, part_sem).wait()


def closing_kernel(pos, mid, mine_a, theirs_a, mine_b, theirs_b, gain, out_ref, *scratch):
    stream, parts, out, in_sem, out_sem = scratch
    tiles = mid.shape[0] // TILE
    near = (pos[2] + pos[3]) & 1

    def arriving(t):
        s = slice(t * TILE, (t + 1) * TILE)
        pairs = [
            (mid.at[s, :HALF], stream.at[near, s, :]),
            (mid.at[s, HALF:], stream.at[1 - near, s, :]),
            (mine_a.at[s, :], parts.at[0, s, :]),
            (theirs_a.at[s, :], parts.at[1, s, :]),
            (mine_b.at[s, :], parts.at[2, s, :]),
        ]
        return [
            pltpu.make_async_copy(src, dst, in_sem.at[t, k]) for k, (src, dst) in enumerate(pairs)
        ]

    for t in range(tiles):
        for c in arriving(t):
            c.start()
    for t in range(tiles):
        for c in arriving(t):
            c.wait()
        for half in range(2):
            s = slice(t * TILE + half * 128, t * TILE + half * 128 + 128)
            a = stream[0, s, :].astype(f32) + (
                parts[0, s, :].astype(f32) + parts[1, s, :].astype(f32)
            )
            b = stream[1, s, :].astype(f32) + (
                parts[2, s, :].astype(f32) + theirs_b[s, :].astype(f32)
            )
            ms = (jnp.sum(a * a, -1, keepdims=True) + jnp.sum(b * b, -1, keepdims=True)) / D
            mine = jnp.where(near == 0, a, b)
            out[s, :] = (mine * lax.rsqrt(ms + epsilon) * gain[...]).astype(bf16)
        s = slice(t * TILE, (t + 1) * TILE)
        pltpu.make_async_copy(out.at[s, :], out_ref.at[s, :], out_sem).start()
    pltpu.make_async_copy(out, out_ref, out_sem).wait()


def cost(flops, moved_bytes):
    return pl.CostEstimate(flops=int(flops), bytes_accessed=int(moved_bytes), transcendentals=0)


def call(kernel, out_shapes, specs, flops, scratch=(), outs=VMEM, room=56):
    return pl.pallas_call(
        kernel,
        out_shape=out_shapes,
        in_specs=specs,
        out_specs=jax.tree.map(lambda _: outs, out_shapes),
        scratch_shapes=list(scratch),
        cost_estimate=cost(flops, 8e6),
        compiler_params=pltpu.CompilerParams(vmem_limit_bytes=room * 2**20),
    )


def flat(pieces, first_col, width, source=0):
    layout = [
        (piece[1], first_col, width, piece[2] if len(piece) > 2 else source) for piece in pieces
    ]
    return [piece[0] for piece in pieces], layout


def local(
    stream_in,
    decay_shift,
    mixer_gain,
    gate_weight,
    input_weight,
    filter_taps,
    recur_gate,
    inlet_gate,
    decay_param,
    mixer_out,
    feedforward_gain,
    up_weight,
    down_weight,
    final_gain,
):
    num_seq, length, half = stream_in.shape
    channels = gate_weight.shape[1]
    hidden = up_weight.shape[1]
    assert num_seq == 1 and half == HALF
    tp = lax.axis_index("tp")
    pos = jnp.stack(
        [lax.axis_index("x"), lax.axis_index("y"), lax.axis_index("z"), tp]
    ).astype(jnp.int32)

    def own_first(gain):
        halves = gain.reshape(2, HALF)
        return jnp.where(tp == 0, halves, halves[::-1]).reshape(1, D)

    own = stream_in.reshape(length, half)
    other = step(own, "tp", 1)

    mid_col, part = hidden // 2, channels // 2
    mixer_t, down_t = mixer_out.T, down_weight.T
    here, wide = [(0, 0, 0, 0, 0)], channels + part
    left = [gate_weight, mixer_t[:, :part], down_t[:, :mid_col]]
    right = [mixer_t[:, part:], input_weight, down_t[:, mid_col:]]
    by_x, at_x = whole_ring(jnp.concatenate(left, axis=1)[None], here, "x")
    by_y, at_y = whole_ring(jnp.concatenate(right, axis=1)[None], here, "y")
    pair, places = both_planes(up_weight)
    by_xy = whole_ring(by_x[:, :, :wide], at_x, "y")
    by_yx = whole_ring(by_y[:, :, :wide], at_y, "x")
    x_pieces = [by_xy, (step(by_xy[0], "z", 1), moved(by_xy[1], "z", 1))]
    y_pieces = [by_yx, (step(by_yx[0], "z", 3), moved(by_yx[1], "z", 1))]

    def later(ring, at, cols, axis):
        both = jnp.concatenate([ring[:, :, wide:], pair[:, :, cols]], axis=0)
        pieces = ring_pieces(both, at + places, axis)
        block = both.shape[1:]
        split = call(
            sort_kernel,
            (jax.ShapeDtypeStruct((16, *block), bf16), jax.ShapeDtypeStruct((8, *block), bf16)),
            [HBM] * 4,
            1e6,
            [pltpu.SemaphoreType.DMA((8,))],
            VMEM,
            16,
        )(*[v for v, _ in pieces])
        return [
            (v, sum((p[s] for _, p in pieces), []))
            for v, s in zip(split, (slice(0, 4), slice(4, 6)))
        ]

    down_a, up_a = later(by_x, at_x, slice(0, mid_col), "y")
    down_b, up_b = later(by_y, at_y, slice(mid_col, hidden), "x")
    up_x = ring_pieces(*up_a, "x")
    up_y = ring_pieces(*up_b, "y")
    far_a = (step(down_a[0], "z", 1), moved(down_a[1], "z", 1))
    far_b = (step(down_b[0], "z", 3), moved(down_b[1], "z", 1))

    shape = jax.ShapeDtypeStruct
    whole, one_half = shape((length, D), bf16), shape((length, HALF), bf16)
    normed = call(norm_kernel, whole, [VMEM] * 3, 2e9, room=24)(own, other, own_first(mixer_gain))

    scan_buffer = pltpu.VMEM((channels // 128, length, 128), f32)
    a, la = flat(x_pieces, 0, channels)
    b, lb = flat(y_pieces, channels, channels, part)
    c, lc = flat(x_pieces, 0, part, channels)
    d, ld = flat(y_pieces, part, part)
    partial = shape((2, length, HALF), bf16)
    mine = call(
        functools.partial(mixer_kernel, la + lb, lc + ld),
        partial,
        [SMEM] + [VMEM] * 6 + [HBM] * len(la + lb + lc + ld),
        1.2e10,
        [
            pltpu.VMEM((D, 2 * channels), bf16),
            pltpu.VMEM((length, channels), bf16),
            pltpu.VMEM((length + 8, channels), f32),
            scan_buffer,
            scan_buffer,
            scan_buffer,
            pltpu.VMEM((D, channels), bf16),
            pltpu.VMEM((2, length, HALF), bf16),
            pltpu.SemaphoreType.DMA,
            pltpu.SemaphoreType.DMA,
            pltpu.SemaphoreType.DMA,
        ],
        HBM,
    )(
        pos,
        normed,
        filter_taps,
        recur_gate,
        inlet_gate,
        (rate_scale * jax.nn.softplus(-decay_param)).reshape(1, channels),
        decay_shift.reshape(length, 1),
        *a,
        *b,
        *c,
        *d,
    )
    theirs = step(mine, "tp", 1)
    tiles = length // TILE

    def halves(low, high):
        (a, la), (b, lb) = flat(low, 0, mid_col), flat(high, mid_col, mid_col)
        return a + b, la + lb

    def turned(left, low, high, plane):
        arrays, layout = halves(low, high)
        return call(
            functools.partial(turned_kernel, layout, plane),
            one_half,
            [SMEM, HBM] + [HBM] * len(layout),
            2 * length * left.shape[1] * HALF,
            [
                pltpu.VMEM(left.shape, bf16),
                pltpu.VMEM((HALF, left.shape[1]), bf16),
                pltpu.SemaphoreType.DMA,
                pltpu.SemaphoreType.DMA((tiles,)),
            ],
            VMEM,
            24,
        )(pos, left, *arrays)

    a, la = flat(up_x, 0, mid_col)
    b, lb = flat(up_y, mid_col, mid_col)
    c, lc = halves([down_a], [down_b])
    mid, activated, mine_c = call(
        functools.partial(ffn_kernel, la + lb, lc),
        (whole, shape((length, hidden), bf16), one_half),
        [SMEM] + [HBM] * 4 + [VMEM] + [HBM] * len(la + lb + lc),
        3 * length * hidden * D,
        [
            pltpu.VMEM((2, length, HALF), bf16),
            pltpu.VMEM((2, 2, length, HALF), bf16),
            pltpu.VMEM((D, hidden), bf16),
            pltpu.VMEM((HALF, hidden), bf16),
            pltpu.VMEM((TILE, D), bf16),
            pltpu.VMEM((length, D), bf16),
            pltpu.VMEM((length, hidden), bf16),
            pltpu.VMEM((length, HALF), bf16),
            pltpu.SemaphoreType.DMA,
            pltpu.SemaphoreType.DMA,
            pltpu.SemaphoreType.DMA((tiles, 6)),
            pltpu.SemaphoreType.DMA,
            pltpu.SemaphoreType.DMA,
            pltpu.SemaphoreType.DMA,
        ],
        HBM,
    )(pos, own, other, mine, theirs, own_first(feedforward_gain), *a, *b, *c)
    theirs_c = step(mine_c, "tp", 1)
    mine_d = turned(activated, [far_a], [far_b], 1)
    theirs_d = step(mine_d, "tp", 1)
    out = call(
        closing_kernel,
        one_half,
        [SMEM] + [HBM] * 4 + [VMEM] * 2,
        2e9,
        [
            pltpu.VMEM((2, length, HALF), bf16),
            pltpu.VMEM((3, length, HALF), bf16),
            pltpu.VMEM((length, HALF), bf16),
            pltpu.SemaphoreType.DMA((tiles, 5)),
            pltpu.SemaphoreType.DMA,
        ],
        HBM,
        24,
    )(pos, mid, mine_c, theirs_c, mine_d, theirs_d, final_gain.reshape(1, HALF))
    return out.reshape(num_seq, length, half)


def solution(mesh):
    grid = Mesh(mesh.devices.reshape(2, 2, 4, 4, 2), ("rep", "z", "y", "x", "tp"))
    fs = ("z", "y", "x")
    seqs = ("rep",) + fs
    return jax.shard_map(
        local,
        mesh=grid,
        in_specs=(
            P(seqs, None, "tp"),
            P(seqs, None),
            P(),
            P(fs, "tp"),
            P(fs, "tp"),
            P(None, "tp"),
            P("tp", None, None),
            P("tp", None, None),
            P("tp"),
            P("tp", fs),
            P(),
            P(fs, "tp"),
            P("tp", fs),
            P("tp"),
        ),
        out_specs=P(seqs, None, "tp"),
        check_vma=False,
    )
```

```python
import functools

import jax
import jax.numpy as jnp
from jax import lax
from jax.experimental import pallas as pl
from jax.experimental.pallas import tpu as pltpu
from jax.sharding import Mesh, PartitionSpec as P

D = 2048
HALF = 1024
ROWS = 64
TILE = 256
SEGS = 8

epsilon = 1e-06
rate_scale = 8.0


f32, bf16 = jnp.float32, jnp.bfloat16
VMEM = pl.BlockSpec(memory_space=pltpu.VMEM)
HBM = pl.BlockSpec(memory_space=pltpu.HBM)
SMEM = pl.BlockSpec(memory_space=pltpu.SMEM)


def step(v, axis, shift):
    size = 2 if axis == "tp" else 4
    over = ("rep", "z") if axis == "z" else axis
    return lax.ppermute(v, over, [(i, (i + shift) % size) for i in range(size)])


def moved(places, axis, by):
    at = "xyz".index(axis)
    return [p[:at] + (p[at] + by,) + p[at + 1 :] for p in places]


def both_planes(shard):
    half = shard.shape[0] // 2
    lower = step(shard[:half], "z", 1)
    upper = step(shard[half:], "z", 3)
    pair = jnp.stack([shard, jnp.concatenate([lower, upper], axis=0)])
    return pair, [(0, 0, 0, 0, 0), (0, 0, 1, 0, 0)]


def ring_pieces(v, places, axis):
    far = step(v, axis, 2)
    left = step(v, axis, 1)
    right = step(v, axis, 3)
    return [
        (v, places),
        (left, moved(places, axis, -1)),
        (right, moved(places, axis, 1)),
        (far, moved(places, axis, 2)),
    ]


def whole_ring(v, places, axis):
    pieces = ring_pieces(v, places, axis)
    whole = jnp.concatenate([p for p, _ in pieces], axis=0)
    return whole, sum((q for _, q in pieces), [])


def start_weights(refs, layout, pos, target, sem, plane=None):
    x, y, z, tp = pos[0], pos[1], pos[2], pos[3]
    for ref, (places, first_col, width, source_col) in zip(refs, layout):
        cols, source = pl.ds(first_col, width), pl.ds(source_col, width)
        for b, (px, py, pz, absolute, first_row) in enumerate(places):
            line = (py * 4 + px) if absolute else ((y + py) & 3) * 4 + ((x + px) & 3)
            at = line * ROWS + first_row
            if plane is None:
                at = ((z + pz + tp) & 1) * HALF + at
            elif pz != plane:
                continue
            at = at if isinstance(at, int) else pl.multiple_of(at, 16)
            pltpu.make_async_copy(
                ref.at[b, :, source], target.at[pl.ds(at, ref.shape[1]), cols], sem
            ).start()


def norm_kernel(own, other, gain, normed):
    def rows(i, _):
        s = pl.ds(pl.multiple_of(i * TILE, TILE), TILE)
        a, b = own[s, :].astype(f32), other[s, :].astype(f32)
        ms = (jnp.sum(a * a, -1, keepdims=True) + jnp.sum(b * b, -1, keepdims=True)) / D
        r = lax.rsqrt(ms + epsilon)
        normed[s, :HALF] = (a * r * gain[:, :HALF]).astype(bf16)
        normed[s, HALF:] = (b * r * gain[:, HALF:]).astype(bf16)
        return 0

    lax.fori_loop(0, own.shape[0] // TILE, rows, 0)


def mixer_kernel(in_layout, out_layout, *refs):
    n, m = len(in_layout), len(out_layout)
    pos, normed, taps, recur_gate, inlet_gate, rate, shift = refs[:7]
    in_pieces, out_pieces, part_out = refs[7 : 7 + n], refs[7 + n : 7 + n + m], refs[7 + n + m]
    entry, gate, padded, decay, drive, prod, weights, part = refs[8 + n + m : -3]
    in_sem, weight_sem, out_sem = refs[-3:]
    length, channels = gate.shape
    start_weights(in_pieces, in_layout, pos, entry, in_sem)
    start_weights(out_pieces, out_layout, pos, weights, weight_sem)
    padded[:8, :] = jnp.zeros((8, channels), f32)
    blocks, block = recur_gate.shape[0], recur_gate.shape[1]
    pltpu.make_async_copy(entry, entry, in_sem).wait()

    def enter(i, _):
        s = pl.ds(pl.multiple_of(i * TILE, TILE), TILE)
        both = jnp.dot(normed[s, :], entry[...], preferred_element_type=f32).astype(bf16)
        gate[s, :] = both[:, :channels]
        padded[pl.ds(pl.multiple_of(8 + i * TILE, 8), TILE), :] = both[:, channels:].astype(f32)
        window = padded[pl.ds(pl.multiple_of(i * TILE, TILE), TILE + 8), :]
        acc = window[5 : 5 + TILE, :] * taps[0:1, :]
        for k in range(1, 4):
            acc = acc + window[5 + k : 5 + k + TILE, :] * taps[k : k + 1, :]
        filt = acc.astype(bf16)
        for n_b in range(blocks):
            cols = slice(n_b * block, (n_b + 1) * block)
            fb = filt[:, cols]
            recur = jax.nn.sigmoid(jnp.dot(fb, recur_gate[n_b], preferred_element_type=f32))
            inlet = jax.nn.sigmoid(jnp.dot(fb, inlet_gate[n_b], preferred_element_type=f32))
            log_decay = shift[s, :] - recur * rate[:, cols]
            a = jnp.exp(log_decay)
            t = 2.0 * log_decay
            series = 1.0 / 120 + t * (1.0 / 720 + t / 5040)
            series = 1.0 / 2 + t * (1.0 / 6 + t * (1.0 / 24 + t * series))
            series = -t * (1.0 + t * series)
            gone = jnp.where(t > -0.4, series, 1.0 - a * a)
            into = jnp.sqrt(gone) * inlet * fb.astype(f32)
            for q in range(block // 128):
                at = n_b * (block // 128) + q
                decay[at, s, :] = a[:, q * 128 : q * 128 + 128]
                drive[at, s, :] = into[:, q * 128 : q * 128 + 128]
        return 0

    lax.fori_loop(0, length // TILE, enter, 0)
    seg = length // SEGS

    def scan(j, carry):
        h, p = carry
        s = pl.ds(j, SEGS, stride=seg)
        hs, ps = [], []
        for q in range(channels // 128):
            a = decay[q, s, :]
            hq = a * h[q] + drive[q, s, :]
            pq = a * p[q]
            drive[q, s, :] = hq
            prod[q, s, :] = pq
            hs.append(hq)
            ps.append(pq)
        return tuple(hs), tuple(ps)

    lanes = channels // 128
    zero, one = jnp.zeros((SEGS, 128), f32), jnp.ones((SEGS, 128), f32)
    lax.fori_loop(0, seg, scan, ((zero,) * lanes, (one,) * lanes), unroll=8)
    pltpu.make_async_copy(weights, weights, weight_sem).wait()

    def leave(r, carry):
        carry, rows = list(carry), []
        for i in range(TILE // seg):
            s = pl.ds(pl.multiple_of(r * TILE + i * seg, seg), seg)
            row = []
            for q in range(lanes):
                states = drive[q, s, :] + prod[q, s, :] * carry[q]
                carry[q] = states[seg - 1 : seg, :]
                branch = jax.nn.gelu(
                    gate[s, q * 128 : q * 128 + 128].astype(f32), approximate=True
                )
                row.append((states * branch).astype(bf16))
            rows.append(jnp.concatenate(row, axis=1))
        left = jnp.concatenate(rows, axis=0)
        s = pl.ds(pl.multiple_of(r * TILE, TILE), TILE)
        for h in range(2):
            half = weights[h * HALF : h * HALF + HALF, :]
            part[h, s, :] = dot_turned(left, half).astype(bf16)
            pltpu.make_async_copy(part.at[h, s, :], part_out.at[h, s, :], out_sem).start()
        return tuple(carry)

    lax.fori_loop(0, length // TILE, leave, (jnp.zeros((1, 128), f32),) * lanes)
    pltpu.make_async_copy(part, part_out, out_sem).wait()


def turned_kernel(layout, plane, *refs):
    n = len(layout)
    pos, left_in = refs[:2]
    pieces, out = refs[2 : 2 + n], refs[2 + n]
    left, weights, sem, in_sem = refs[3 + n :]
    tiles = out.shape[0] // TILE

    def arriving(t):
        s = pl.ds(pl.multiple_of(t * TILE, TILE), TILE)
        return pltpu.make_async_copy(left_in.at[s, :], left.at[s, :], in_sem.at[t])

    arriving(0).start()
    start_weights(pieces, layout, pos, weights, sem, plane)
    for t in range(1, tiles):
        arriving(t).start()
    pltpu.make_async_copy(weights, weights, sem).wait()

    def rows(t, _):
        arriving(t).wait()
        s = pl.ds(pl.multiple_of(t * TILE, TILE), TILE)
        out[s, :] = dot_turned(left[s, :], weights[...]).astype(bf16)
        return 0

    lax.fori_loop(0, tiles, rows, 0)


def dot_turned(left, right):
    return lax.dot_general(left, right, (((1,), (1,)), ((), ())), preferred_element_type=f32)


def ffn_kernel(layout, down_layout, *refs):
    pos, own, other, mine, theirs, gain = refs[:6]
    n, m = len(layout), len(down_layout)
    pieces, down_pieces = refs[6 : 6 + n], refs[6 + n : 6 + n + m]
    mid_out, act_out, part_out = refs[6 + n + m : 9 + n + m]
    stream, parts, up, down, normed, mid, act, part = refs[9 + n + m : 17 + n + m]
    up_sem, down_sem, in_sem, act_sem, mid_sem, part_sem = refs[17 + n + m :]
    tiles = own.shape[0] // TILE

    def arriving(t):
        s = pl.ds(pl.multiple_of(t * TILE, TILE), TILE)
        pairs = [
            (own, stream.at[0]),
            (other, stream.at[1]),
            (mine.at[0], parts.at[0, 0]),
            (theirs.at[1], parts.at[0, 1]),
            (mine.at[1], parts.at[1, 0]),
            (theirs.at[0], parts.at[1, 1]),
        ]
        return [
            pltpu.make_async_copy(src.at[s, :], dst.at[s, :], in_sem.at[t, k])
            for k, (src, dst) in enumerate(pairs)
        ]

    for c in arriving(0):
        c.start()
    start_weights(pieces, layout, pos, up, up_sem)
    for c in arriving(1):
        c.start()
    start_weights(down_pieces, down_layout, pos, down, down_sem, 0)
    for t in range(2, tiles):
        for c in arriving(t):
            c.start()

    def rows(t, _):
        for c in arriving(t):
            c.wait()
        s = pl.ds(pl.multiple_of(t * TILE, TILE), TILE)
        halves = []
        for h in range(2):
            v = stream[h, s, :].astype(f32) + (
                parts[h, 0, s, :].astype(f32) + parts[h, 1, s, :].astype(f32)
            )
            v = v.astype(bf16)
            mid[s, h * HALF : h * HALF + HALF] = v
            halves.append(v.astype(f32))
        a, b = halves
        ms = (jnp.sum(a * a, -1, keepdims=True) + jnp.sum(b * b, -1, keepdims=True)) / D
        r = lax.rsqrt(ms + epsilon)
        normed[:, :HALF] = (a * r * gain[:, :HALF]).astype(bf16)
        normed[:, HALF:] = (b * r * gain[:, HALF:]).astype(bf16)
        pltpu.make_async_copy(mid.at[s, :], mid_out.at[s, :], mid_sem).start()

        @pl.when(t == 0)
        def _():
            pltpu.make_async_copy(up, up, up_sem).wait()
            pltpu.make_async_copy(down, down, down_sem).wait()

        prod = jnp.dot(normed[...], up[...], preferred_element_type=f32)
        left = jnp.square(jnp.maximum(prod, 0.0)).astype(bf16)
        act[s, :] = left
        pltpu.make_async_copy(act.at[s, :], act_out.at[s, :], act_sem).start()
        part[s, :] = dot_turned(left, down[...]).astype(bf16)
        pltpu.make_async_copy(part.at[s, :], part_out.at[s, :], part_sem).start()
        return 0

    lax.fori_loop(0, tiles, rows, 0)
    pltpu.make_async_copy(mid, mid_out, mid_sem).wait()
    pltpu.make_async_copy(act, act_out, act_sem).wait()
    pltpu.make_async_copy(part, part_out, part_sem).wait()


def closing_kernel(pos, mid, mine_a, theirs_a, mine_b, theirs_b, gain, out_ref, *scratch):
    stream, parts, out, in_sem, out_sem = scratch
    tiles = mid.shape[0] // TILE
    near = (pos[2] + pos[3]) & 1

    def arriving(t):
        s = slice(t * TILE, (t + 1) * TILE)
        pairs = [
            (mid.at[s, :HALF], stream.at[near, s, :]),
            (mid.at[s, HALF:], stream.at[1 - near, s, :]),
            (mine_a.at[s, :], parts.at[0, s, :]),
            (theirs_a.at[s, :], parts.at[1, s, :]),
            (mine_b.at[s, :], parts.at[2, s, :]),
        ]
        return [
            pltpu.make_async_copy(src, dst, in_sem.at[t, k]) for k, (src, dst) in enumerate(pairs)
        ]

    for t in range(tiles):
        for c in arriving(t):
            c.start()
    for t in range(tiles):
        for c in arriving(t):
            c.wait()
        for half in range(2):
            s = slice(t * TILE + half * 128, t * TILE + half * 128 + 128)
            a = stream[0, s, :].astype(f32) + (
                parts[0, s, :].astype(f32) + parts[1, s, :].astype(f32)
            )
            b = stream[1, s, :].astype(f32) + (
                parts[2, s, :].astype(f32) + theirs_b[s, :].astype(f32)
            )
            ms = (jnp.sum(a * a, -1, keepdims=True) + jnp.sum(b * b, -1, keepdims=True)) / D
            mine = jnp.where(near == 0, a, b)
            out[s, :] = (mine * lax.rsqrt(ms + epsilon) * gain[...]).astype(bf16)
        s = slice(t * TILE, (t + 1) * TILE)
        pltpu.make_async_copy(out.at[s, :], out_ref.at[s, :], out_sem).start()
    pltpu.make_async_copy(out, out_ref, out_sem).wait()


def cost(flops, moved_bytes):
    return pl.CostEstimate(flops=int(flops), bytes_accessed=int(moved_bytes), transcendentals=0)


def call(kernel, out_shapes, specs, flops, scratch=(), outs=VMEM, room=56):
    return pl.pallas_call(
        kernel,
        out_shape=out_shapes,
        in_specs=specs,
        out_specs=jax.tree.map(lambda _: outs, out_shapes),
        scratch_shapes=list(scratch),
        cost_estimate=cost(flops, 8e6),
        compiler_params=pltpu.CompilerParams(vmem_limit_bytes=room * 2**20),
    )


def flat(pieces, first_col, width, source=0):
    layout = [
        (piece[1], first_col, width, piece[2] if len(piece) > 2 else source) for piece in pieces
    ]
    return [piece[0] for piece in pieces], layout


def local(
    stream_in,
    decay_shift,
    mixer_gain,
    gate_weight,
    input_weight,
    filter_taps,
    recur_gate,
    inlet_gate,
    decay_param,
    mixer_out,
    feedforward_gain,
    up_weight,
    down_weight,
    final_gain,
):
    num_seq, length, half = stream_in.shape
    channels = gate_weight.shape[1]
    hidden = up_weight.shape[1]
    assert num_seq == 1 and half == HALF
    tp = lax.axis_index("tp")
    pos = jnp.stack(
        [lax.axis_index("x"), lax.axis_index("y"), lax.axis_index("z"), tp]
    ).astype(jnp.int32)

    def own_first(gain):
        halves = gain.reshape(2, HALF)
        return jnp.where(tp == 0, halves, halves[::-1]).reshape(1, D)

    own = stream_in.reshape(length, half)
    other = step(own, "tp", 1)

    mid_col, part = hidden // 2, channels // 2
    mixer_t, down_t = mixer_out.T, down_weight.T
    here, wide = [(0, 0, 0, 0, 0)], channels + part
    left = [gate_weight, mixer_t[:, :part], down_t[:, :mid_col]]
    right = [mixer_t[:, part:], input_weight, down_t[:, mid_col:]]
    by_x, at_x = whole_ring(jnp.concatenate(left, axis=1)[None], here, "x")
    by_y, at_y = whole_ring(jnp.concatenate(right, axis=1)[None], here, "y")
    pair, places = both_planes(up_weight)
    by_xy = whole_ring(by_x[:, :, :wide], at_x, "y")
    by_yx = whole_ring(by_y[:, :, :wide], at_y, "x")
    x_pieces = [by_xy, (step(by_xy[0], "z", 1), moved(by_xy[1], "z", 1))]
    y_pieces = [by_yx, (step(by_yx[0], "z", 3), moved(by_yx[1], "z", 1))]

    up_a = whole_ring(pair[:, :, :mid_col], places, "y")
    up_b = whole_ring(pair[:, :, mid_col:], places, "x")
    down_a = whole_ring(by_x[:, :, wide:], at_x, "y")
    down_b = whole_ring(by_y[:, :, wide:], at_y, "x")
    up_x = ring_pieces(*up_a, "x")
    up_y = ring_pieces(*up_b, "y")
    far_a = (step(down_a[0], "z", 1), moved(down_a[1], "z", 1))
    far_b = (step(down_b[0], "z", 3), moved(down_b[1], "z", 1))

    shape = jax.ShapeDtypeStruct
    whole, one_half = shape((length, D), bf16), shape((length, HALF), bf16)
    normed = call(norm_kernel, whole, [VMEM] * 3, 2e9, room=24)(own, other, own_first(mixer_gain))

    scan_buffer = pltpu.VMEM((channels // 128, length, 128), f32)
    a, la = flat(x_pieces, 0, channels)
    b, lb = flat(y_pieces, channels, channels, part)
    c, lc = flat(x_pieces, 0, part, channels)
    d, ld = flat(y_pieces, part, part)
    partial = shape((2, length, HALF), bf16)
    mine = call(
        functools.partial(mixer_kernel, la + lb, lc + ld),
        partial,
        [SMEM] + [VMEM] * 6 + [HBM] * len(la + lb + lc + ld),
        1.2e10,
        [
            pltpu.VMEM((D, 2 * channels), bf16),
            pltpu.VMEM((length, channels), bf16),
            pltpu.VMEM((length + 8, channels), f32),
            scan_buffer,
            scan_buffer,
            scan_buffer,
            pltpu.VMEM((D, channels), bf16),
            pltpu.VMEM((2, length, HALF), bf16),
            pltpu.SemaphoreType.DMA,
            pltpu.SemaphoreType.DMA,
            pltpu.SemaphoreType.DMA,
        ],
        HBM,
        40,
    )(
        pos,
        normed,
        filter_taps,
        recur_gate,
        inlet_gate,
        (rate_scale * jax.nn.softplus(-decay_param)).reshape(1, channels),
        decay_shift.reshape(length, 1),
        *a,
        *b,
        *c,
        *d,
    )
    theirs = step(mine, "tp", 1)
    tiles = length // TILE

    def halves(low, high):
        (a, la), (b, lb) = flat(low, 0, mid_col), flat(high, mid_col, mid_col)
        return a + b, la + lb

    def turned(left, low, high, plane):
        arrays, layout = halves(low, high)
        return call(
            functools.partial(turned_kernel, layout, plane),
            one_half,
            [SMEM, HBM] + [HBM] * len(layout),
            2 * length * left.shape[1] * HALF,
            [
                pltpu.VMEM(left.shape, bf16),
                pltpu.VMEM((HALF, left.shape[1]), bf16),
                pltpu.SemaphoreType.DMA,
                pltpu.SemaphoreType.DMA((tiles,)),
            ],
            VMEM,
            24,
        )(pos, left, *arrays)

    a, la = flat(up_x, 0, mid_col)
    b, lb = flat(up_y, mid_col, mid_col)
    c, lc = halves([down_a], [down_b])
    mid, activated, mine_c = call(
        functools.partial(ffn_kernel, la + lb, lc),
        (whole, shape((length, hidden), bf16), one_half),
        [SMEM] + [HBM] * 4 + [VMEM] + [HBM] * len(la + lb + lc),
        3 * length * hidden * D,
        [
            pltpu.VMEM((2, length, HALF), bf16),
            pltpu.VMEM((2, 2, length, HALF), bf16),
            pltpu.VMEM((D, hidden), bf16),
            pltpu.VMEM((HALF, hidden), bf16),
            pltpu.VMEM((TILE, D), bf16),
            pltpu.VMEM((length, D), bf16),
            pltpu.VMEM((length, hidden), bf16),
            pltpu.VMEM((length, HALF), bf16),
            pltpu.SemaphoreType.DMA,
            pltpu.SemaphoreType.DMA,
            pltpu.SemaphoreType.DMA((tiles, 6)),
            pltpu.SemaphoreType.DMA,
            pltpu.SemaphoreType.DMA,
            pltpu.SemaphoreType.DMA,
        ],
        HBM,
    )(pos, own, other, mine, theirs, own_first(feedforward_gain), *a, *b, *c)
    theirs_c = step(mine_c, "tp", 1)
    mine_d = turned(activated, [far_a], [far_b], 1)
    theirs_d = step(mine_d, "tp", 1)
    out = call(
        closing_kernel,
        one_half,
        [SMEM] + [HBM] * 4 + [VMEM] * 2,
        2e9,
        [
            pltpu.VMEM((2, length, HALF), bf16),
            pltpu.VMEM((3, length, HALF), bf16),
            pltpu.VMEM((length, HALF), bf16),
            pltpu.SemaphoreType.DMA((tiles, 5)),
            pltpu.SemaphoreType.DMA,
        ],
        HBM,
        24,
    )(pos, mid, mine_c, theirs_c, mine_d, theirs_d, final_gain.reshape(1, HALF))
    return out.reshape(num_seq, length, half)


def solution(mesh):
    grid = Mesh(mesh.devices.reshape(2, 2, 4, 4, 2), ("rep", "z", "y", "x", "tp"))
    fs = ("z", "y", "x")
    seqs = ("rep",) + fs
    return jax.shard_map(
        local,
        mesh=grid,
        in_specs=(
            P(seqs, None, "tp"),
            P(seqs, None),
            P(),
            P(fs, "tp"),
            P(fs, "tp"),
            P(None, "tp"),
            P("tp", None, None),
            P("tp", None, None),
            P("tp"),
            P("tp", fs),
            P(),
            P(fs, "tp"),
            P("tp", fs),
            P("tp"),
        ),
        out_specs=P(seqs, None, "tp"),
        check_vma=False,
    )
```
